256 devices in a mesh: fs: 64 (over z, x, core), tp: 4 (over y).
Axes of the slice: x: 4, y: 4, z: 8, core: 2. Of those that a mesh axis runs over, the one named last changes fastest.
Arguments:
- tokens: bfloat16 [65536, 2048], P('fs', 'tp'), may hold values from -50 to 50
- norm_gain: float32 [2048], P('fs'), may hold values from 0.1 to 1.9
- gate_weight: float32 [2048, 2816], P('fs', 'tp'), may hold values from -0.125 to 0.125
- up_weight: float32 [2048, 2816], P('fs', 'tp'), may hold values from -0.125 to 0.125
- down_weight: float32 [2816, 2048], P('fs', 'tp'), may hold values from -0.109375 to 0.109375
Outputs:
- gate_sampler: bfloat16 [2048, 2816], P(None, 'tp')
- up_sampler: bfloat16 [2048, 2816], P(None, 'tp')
- down_sampler: bfloat16 [2816, 2048], P('tp')
- mixed: bfloat16 [65536, 2048], P('fs', 'tp')
The draws below stay inside these ranges and needn't reach their ends.
All inputs are finite; a program needn't handle non-finite values.
Results may differ from the reference program's by a relative error of at most 0.0095.
Values may be sent and summed in bfloat16 or wider, within the bound.
A program may use at most 128 MiB of HBM per device.

```python
import math
import jax
import jax.numpy as jnp
from jax import lax

D = 2048
FF = 2816
TOKENS = 65536
HID_DEV = 704
N_TP = 4


def draw_tokens(key, part):
    first, second, third = jax.random.split(key, 3)
    row_scale = jnp.exp(jax.random.uniform(first, (TOKENS, 1), jnp.float32, 0.0, math.log(10.0)))
    col_scale = jnp.exp(jax.random.uniform(second, (1, D), jnp.float32, 0.0, math.log(10.0)))
    base = jnp.clip(jax.random.normal(third, (TOKENS, D), jnp.float32), -5.0, 5.0)
    return (base * row_scale * col_scale / 10.0).astype(jnp.bfloat16)


def steps_of(key, shape, cuts, low, high):
    gain, own = 1.0, jax.random.fold_in(key, 6)
    for axis_at, shards_of in cuts:
        steps = jnp.exp(jax.random.uniform(jax.random.fold_in(own, axis_at), (shards_of,), jnp.float32, low / len(cuts), high / len(cuts)))
        gain = gain * jnp.repeat(steps, shape[axis_at] // shards_of).reshape([-1 if axis == axis_at else 1 for axis in range(len(shape))])
    return gain


def gaussian(rng, shape, scale, limit, cuts=(), held_as=jnp.bfloat16):
    factor_of = steps_of(rng, shape, cuts, -0.22, 0.18) if cuts else 1.0
    values = jax.random.normal(rng, shape, jnp.float32) * scale * factor_of
    return jnp.minimum(jnp.maximum(values, -limit), limit).astype(held_as)


def setup_inputs(seed: int = 0) -> dict:
    key_of = jax.random.split(jax.random.key(seed), 6)
    return {
        "tokens": draw_tokens(jax.random.fold_in(key_of[5], 71), 0),
        "norm_gain": jnp.clip(1.0 + 0.18 * jax.random.normal(key_of[1], (D,), jnp.float32), 0.1, 1.9),
        "gate_weight": gaussian(key_of[2], (D, FF), D ** -0.5, 0.125, ((0, 64), (1, 4)), jnp.float32),
        "up_weight": gaussian(key_of[3], (D, FF), D ** -0.5, 0.125, ((0, 64), (1, 4)), jnp.float32),
        "down_weight": gaussian(key_of[4], (FF, D), FF ** -0.5, 0.109375, ((0, 64), (1, 4)), jnp.float32),
    }


norm_eps = 1e-06

def reference(tokens, norm_gain, gate_weight, up_weight, down_weight):
    gate_sampler = (norm_gain[:, None] * gate_weight).astype(jnp.bfloat16)
    up_sampler = (norm_gain[:, None] * up_weight).astype(jnp.bfloat16)
    down_sampler = down_weight.astype(jnp.bfloat16)
    floated = tokens.astype(jnp.float32)
    normed = (floated * lax.rsqrt(lax.optimization_barrier(jnp.mean(floated * floated, axis=-1, keepdims=True)) + norm_eps)).astype(jnp.bfloat16)
    gate = jnp.dot(normed, gate_sampler, preferred_element_type=jnp.float32)
    up = jnp.dot(normed, up_sampler, preferred_element_type=jnp.float32)
    hidden = (jax.nn.silu(gate) * up).astype(jnp.bfloat16)
    summed = jnp.zeros((tokens.shape[0], tokens.shape[1]), jnp.float32)
    for block_index in range(N_TP):
        low = block_index * HID_DEV
        partial_value = jnp.dot(hidden[:, low:low + HID_DEV], down_sampler[low:low + HID_DEV, :], preferred_element_type=jnp.float32).astype(jnp.bfloat16)
        partial_value = lax.optimization_barrier(partial_value)
        summed = summed + partial_value.astype(jnp.float32)
    return (gate_sampler, up_sampler, down_sampler, summed.astype(jnp.bfloat16))
```

```python
import functools

import jax
import jax.numpy as jnp
from jax import lax
from jax.experimental import pallas as pl
from jax.experimental.pallas import tpu as pltpu
from jax.sharding import PartitionSpec as P

MESH = pl.DeviceIdType.MESH
BF = jnp.bfloat16
F32 = jnp.float32
NZ, NX, NC, NY = 8, 4, 2, 4
ROWS = 32
HID = 704
WIDE = 768
DROWS, COLS = 44, 512
D = 2048
CHUNK, CHUNKS = 256, 4
HALF = CHUNK // 2
EPS = 1e-06


def kernel(
    tok, gain, gw, uw, dw,
    go, uo, do, mo,
    xs, sg, sud, dsend, df, tmp, gst, ust, xn, hid, part, far, near, comb, sums, out,
    ps, pr, gxs, gxr, gzs, gzr, us, ur, uxs, uxr, ufs, ufr, ds_, dr, ts, tr, tfs, tfr, rs, rr, loc,
):
    f, y = lax.axis_index("fs"), lax.axis_index("tp")
    z, x, c = f // 8, (f // 2) % 4, f % 2
    za, zb = z // 2, z % 2

    def at(zz, xx, cc, yy):
        return ((zz * NX + xx) * NC + cc, yy)

    zp, zm = (z + 1) % NZ, (z + 7) % NZ
    xp, xm, x2 = (x + 1) % NX, (x + 3) % NX, (x + 2) % NX
    yp, ym, y2 = (y + 1) % NY, (y + 3) % NY, (y + 2) % NY
    z_next, z_prev = at(zp, x, c, y), at(zm, x, c, y)
    x_next, x_prev, x_far = at(z, xp, c, y), at(z, xm, c, y), at(z, x2, c, y)
    y_next, y_prev = at(z, x, c, yp), at(z, x, c, ym)
    twin = at(z, x, 1 - c, y)
    pz = 2 * y + zb
    swap = at(pz, x, c, za)
    moves = za != y

    def remote(src, dst, send, recv, device):
        return pltpu.make_async_remote_copy(
            src_ref=src, dst_ref=dst, send_sem=send, recv_sem=recv, device_id=device, device_id_type=MESH
        )

    eye = lax.broadcasted_iota(jnp.int32, (ROWS, ROWS), 0) == lax.broadcasted_iota(jnp.int32, (ROWS, ROWS), 1)
    scale = jnp.sum(jnp.where(eye, jnp.broadcast_to(gain[...], (ROWS, ROWS)), 0.0), axis=1, keepdims=True)
    tail = jnp.zeros((ROWS, WIDE - HID), F32)
    sg[z, x, c] = jnp.concatenate([scale * gw[...], tail], axis=1).astype(BF)
    sud[z, x, c, 0] = jnp.concatenate([scale * uw[...], tail], axis=1).astype(BF)
    low = jnp.concatenate([dw[pl.ds(ROWS, DROWS - ROWS), :], jnp.zeros((4, COLS), F32)], axis=0)
    right = jnp.concatenate([low[:, :256], low[:, 256:]], axis=0)
    packed = jnp.concatenate([dw[pl.ds(0, ROWS), :], right], axis=1).astype(BF)

    @pl.when(moves)
    def _():
        dsend[...] = packed

    @pl.when(jnp.logical_not(moves))
    def _():
        sud[z, x, c, 1] = packed

    df[pl.ds(HID, WIDE - HID), :] = jnp.zeros((WIDE - HID, D), BF)

    own_tokens = pltpu.make_async_copy(tok, xs.at[y], loc.at[0])
    own_tokens.start()

    barrier = pltpu.get_barrier_semaphore()
    for partner in (z_next, z_prev, x_next, x_prev, x_far, y_next, y_prev, twin):
        pl.semaphore_signal(barrier, inc=1, device_id=partner, device_id_type=MESH)

    @pl.when(moves)
    def _():
        pl.semaphore_signal(barrier, inc=1, device_id=swap, device_id_type=MESH)

    pl.semaphore_wait(barrier, 8 + moves.astype(jnp.int32))

    sends = []

    def go_(copy):
        copy.start()
        sends.append(copy)

    change = remote(dsend, sud.at[pz, x, c, 1], ps.at[0], pr.at[0], swap)

    @pl.when(moves)
    def _():
        change.start()

    def token_copy(way, j):
        rows = pl.ds(j * CHUNK, CHUNK)
        return remote(
            tok.at[rows], xs.at[y, rows], ts.at[way * CHUNKS + j], tr.at[way * CHUNKS + j], (y_next, y_prev)[way]
        )

    def token_forward(way, j):
        rows = pl.ds(j * CHUNK + way * HALF, HALF)
        block = xs.at[(ym, yp)[way], rows]
        return remote(block, block, tfs.at[way * CHUNKS + j], tfr.at[way * CHUNKS + j], (y_next, y_prev)[way])

    def token_pass(j):
        for way in range(2):
            token_copy(way, j).wait_recv()
            go_(token_forward(way, j))

    for j in range(CHUNKS):
        for way in range(2):
            go_(token_copy(way, j))

    own_gate = sg.at[z, x, c]
    gx = [remote(own_gate, own_gate, gxs.at[k], gxr.at[k], to) for k, to in enumerate((x_next, x_prev, x_far))]
    for copy in gx:
        go_(copy)

    @pl.when(moves)
    def _():
        change.wait_recv()

    def ud_z(way, k):
        block = sud.at[(z + (NZ - k if way == 0 else k)) % NZ, x, c]
        return remote(block, block, us.at[way * 4 + k], ur.at[way * 4 + k], (z_next, z_prev)[way])

    def g_z(way, k, h):
        block = sg.at[(z + (NZ - k if way == 0 else k)) % NZ, pl.ds(2 * h, 2), c]
        n = (way * 4 + k) * 2 + h
        return remote(block, block, gzs.at[n], gzr.at[n], (z_next, z_prev)[way])

    def ud_x(o, way):
        block = sud.at[(z + order[o]) % NZ, x, c]
        return remote(block, block, uxs.at[o * 2 + way], uxr.at[o * 2 + way], (x_next, x_prev)[way])

    def ud_f(o):
        way = turn[o]
        block = sud.at[(z + order[o]) % NZ, (xm, xp)[way], c]
        return remote(block, block, ufs.at[o], ufr.at[o], (x_next, x_prev)[way])

    def twin_copy(n, block):
        return remote(block, block, ds_.at[n], dr.at[n], twin)

    def g_twin(o, cc):
        return twin_copy(o, sg.at[(z + order[o]) % NZ, :, cc])

    def ud_twin(o, cc):
        return twin_copy(8 + o, sud.at[(z + order[o]) % NZ, :, cc])

    order = [0, 7, 1, 6, 2, 5, 3, 4]
    turn = [0, 0, 1, 0, 1, 0, 1, 1]

    def ud_arrived(o):
        for way in range(2):
            go_(ud_x(o, way))

    def x_pass(o):
        for way in range(2):
            ud_x(o, way).wait_recv()
        go_(ud_f(o))

    def x_end(o):
        ud_f(o).wait_recv()
        go_(ud_twin(o, c))

    for way in range(2):
        go_(ud_z(way, 0))
    ud_arrived(0)
    for copy in gx:
        copy.wait_recv()
    for h in range(2):
        for way in range(2):
            go_(g_z(way, 0, h))
    go_(g_twin(0, c))

    last = (4, 3)
    for k in range(1, 5):
        ways = [way for way in range(2) if k <= last[way]]
        for way in ways:
            ud_z(way, k - 1).wait_recv()
            if k < last[way]:
                go_(ud_z(way, k))
            ud_arrived(7 if k == 4 else 2 * k - 1 + way)
        for way in ways:
            for h in range(2):
                g_z(way, k - 1, h).wait_recv()
                if k < last[way]:
                    go_(g_z(way, k, h))
            go_(g_twin(7 if k == 4 else 2 * k - 1 + way, c))
        for o in [[0], [1, 2], [3, 4], [5, 6]][k - 1]:
            x_pass(o)
        for o in [[], [0], [1, 2], [3, 4]][k - 1]:
            x_end(o)
        token_pass(k - 1)
    x_pass(7)
    x_end(5)
    x_end(6)
    x_end(7)
    for o in range(8):
        g_twin(o, 1 - c).wait_recv()
        ud_twin(o, 1 - c).wait_recv()

    def assemble(n, carry):
        a, group = n // 4, n % 4
        for s in range(4):
            shard = sud[2 * a + group // 2, (group % 2) * 2 + s // 2, s % 2, 1].astype(F32)
            tmp[pl.ds(DROWS * s, ROWS), :] = shard[:, :COLS]
            at_row = DROWS * s + ROWS
            tmp[pl.ds(at_row, DROWS - ROWS), pl.ds(0, 256)] = shard[: DROWS - ROWS, COLS:]
            tmp[pl.ds(at_row, DROWS - ROWS), pl.ds(256, 256)] = shard[16 : 16 + DROWS - ROWS, COLS:]
        rows = pl.ds(pl.multiple_of(group * 176, 16), 176)
        df[rows, pl.ds(pl.multiple_of(a * COLS, COLS), COLS)] = tmp[...].astype(BF)
        return carry

    lax.fori_loop(0, 16, assemble, 0)
    own_tokens.wait()

    def message(kind, way, j):
        rows = {"far": 1 - way, "near": way, "comb": 1 - way}[kind]
        to_block = y2 if kind == "far" else (yp, ym)[way]
        src = sums.at[way, j] if kind == "comb" else part.at[j, to_block, pl.ds(rows * HALF, HALF)]
        dst = {"far": far, "near": near, "comb": comb}[kind].at[way, j]
        n = (("far", "near", "comb").index(kind) * 2 + way) * CHUNKS + j
        return remote(src, dst, rs.at[n], rr.at[n], (y_next, y_prev)[way])

    def compute(j):
        for way in range(2):
            token_forward(way, j).wait_recv()

        def normalise(t, carry):
            rows = pl.ds(pl.multiple_of(j * CHUNK + t * 32, 32), 32)
            total = jnp.zeros((32, 1), F32)
            for b in range(NY):
                v = xs[b, rows, :].astype(F32)
                total = total + jnp.sum(v * v, axis=1, keepdims=True)
            r = lax.rsqrt(total / D + EPS)
            for b in range(NY):
                v = xs[b, rows, :].astype(F32)
                xn[pl.ds(pl.multiple_of(t * 32, 32), 32), pl.ds(b * COLS, COLS)] = (v * r).astype(BF)
            return carry

        lax.fori_loop(0, CHUNK // 32, normalise, 0)

        def first(n, carry):
            cols = pl.ds(pl.multiple_of(n * 256, 256), 256)
            gate = jnp.dot(xn[...], sg[:, :, :, :, cols].reshape(D, 256), preferred_element_type=F32)
            up = jnp.dot(xn[...], sud[:, :, :, 0, :, cols].reshape(D, 256), preferred_element_type=F32)
            hid[:, cols] = (gate / (1.0 + jnp.exp(-gate)) * up).astype(BF)
            return carry

        lax.fori_loop(0, WIDE // 256, first, 0)

        def second(n, carry):
            b = (y + 2 + n) % NY
            cols = pl.ds(pl.multiple_of(b * COLS, COLS), COLS)
            part[j, b] = jnp.dot(hid[...], df[:, cols], preferred_element_type=F32).astype(BF)
            return carry

        lax.fori_loop(0, NY, second, 0)
        for kind in ("far", "near"):
            for way in range(2):
                message(kind, way, j).start()

    def combine(j):
        for way in range(2):
            message("far", way, j).wait_recv()
            rows = pl.ds((1 - way) * HALF, HALF)
            mine = part[j, (yp, ym)[way], rows, :].astype(F32)
            sums[way, j] = (mine + far[way, j].astype(F32)).astype(BF)
        for way in range(2):
            message("comb", way, j).start()

    def step(j, carry):
        @pl.when(j < CHUNKS)
        def _():
            compute(j)

        @pl.when(j > 0)
        def _():
            combine(j - 1)

        return carry

    lax.fori_loop(0, CHUNKS + 1, step, 0)

    def narrow(n, carry):
        zz, xx, cc = n // 8, (n // 2) % 4, n % 2
        gst[n] = sg[zz, xx, cc][:, :HID]
        ust[n] = sud[zz, xx, cc, 0][:, :HID]
        return carry

    lax.fori_loop(0, NZ * NX * NC, narrow, 0)
    weights = [
        pltpu.make_async_copy(gst, go, loc.at[1]),
        pltpu.make_async_copy(ust, uo, loc.at[2]),
        pltpu.make_async_copy(df.at[pl.ds(0, HID)], do, loc.at[3]),
    ]
    for copy in weights:
        copy.start()

    def out_copy(j):
        return pltpu.make_async_copy(out.at[j], mo.at[pl.ds(j * CHUNK, CHUNK)], loc.at[4 + j])

    def finish(j, carry):
        for way in range(2):
            message("near", way, j).wait_recv()
            message("comb", way, j).wait_recv()
        for half in range(2):
            rows = pl.ds(half * HALF, HALF)
            mine = part[j, y, rows, :].astype(F32)
            total = mine + near[half, j].astype(F32) + comb[1 - half, j].astype(F32)
            out[j, rows, :] = total.astype(BF)
        out_copy(j).start()
        return carry

    lax.fori_loop(0, CHUNKS, finish, 0)

    for copy in sends:
        copy.wait_send()

    @pl.when(moves)
    def _():
        change.wait_send()

    def drain(j, carry):
        for kind in ("far", "near", "comb"):
            for way in range(2):
                message(kind, way, j).wait_send()
        out_copy(j).wait()
        return carry

    lax.fori_loop(0, CHUNKS, drain, 0)
    for copy in weights:
        copy.wait()


def shards(tokens, norm_gain, gate_weight, up_weight, down_weight):
    vmem = functools.partial(pltpu.VMEM, dtype=BF)
    sem = pltpu.SemaphoreType.DMA
    anywhere = pl.BlockSpec(memory_space=pl.ANY)
    whole = pl.BlockSpec(memory_space=pltpu.VMEM)
    gate, up, down, mixed = pl.pallas_call(
        kernel,
        name="layer",
        out_shape=(
            jax.ShapeDtypeStruct((NZ * NX * NC, ROWS, HID), BF),
            jax.ShapeDtypeStruct((NZ * NX * NC, ROWS, HID), BF),
            jax.ShapeDtypeStruct((HID, D), BF),
            jax.ShapeDtypeStruct((CHUNK * CHUNKS, COLS), BF),
        ),
        in_specs=[anywhere, whole, whole, whole, whole],
        out_specs=(anywhere,) * 4,
        scratch_shapes=[
            vmem((NY, CHUNK * CHUNKS, COLS)),
            vmem((NZ, NX, NC, ROWS, WIDE)),
            vmem((NZ, NX, NC, 2, ROWS, WIDE)),
            vmem((ROWS, WIDE)),
            vmem((WIDE, D)),
            pltpu.VMEM((4 * DROWS, COLS), F32),
            vmem((NZ * NX * NC, ROWS, HID)),
            vmem((NZ * NX * NC, ROWS, HID)),
            vmem((CHUNK, D)),
            vmem((CHUNK, WIDE)),
            vmem((CHUNKS, NY, CHUNK, COLS)),
            vmem((2, CHUNKS, HALF, COLS)),
            vmem((2, CHUNKS, HALF, COLS)),
            vmem((2, CHUNKS, HALF, COLS)),
            vmem((2, CHUNKS, HALF, COLS)),
            vmem((CHUNKS, CHUNK, COLS)),
            sem((1,)), sem((1,)),
            sem((3,)), sem((3,)),
            sem((16,)), sem((16,)),
            sem((8,)), sem((8,)),
            sem((16,)), sem((16,)),
            sem((8,)), sem((8,)),
            sem((16,)), sem((16,)),
            sem((8,)), sem((8,)),
            sem((8,)), sem((8,)),
            sem((24,)), sem((24,)),
            sem((8,)),
        ],
        compiler_params=pltpu.CompilerParams(collective_id=0, has_side_effects=True, vmem_limit_bytes=44 * 2**20),
    )(tokens, norm_gain.reshape(1, ROWS), gate_weight, up_weight, down_weight)
    return (gate.reshape(D, HID), up.reshape(D, HID), down, mixed)


def solution(mesh):
    return jax.shard_map(
        shards,
        mesh=mesh,
        in_specs=(P("fs", "tp"), P("fs"), P("fs", "tp"), P("fs", "tp"), P("fs", "tp")),
        out_specs=(P(None, "tp"), P(None, "tp"), P("tp", None), P("fs", "tp")),
        check_vma=False,
    )
```

```python
import functools

import jax
import jax.numpy as jnp
from jax import lax
from jax.experimental import pallas as pl
from jax.experimental.pallas import tpu as pltpu
from jax.sharding import PartitionSpec as P

MESH = pl.DeviceIdType.MESH
BF = jnp.bfloat16
F32 = jnp.float32
NZ, NX, NC, NY = 8, 4, 2, 4
ROWS = 32
HID = 704
WIDE = 768
DROWS, COLS = 44, 512
D = 2048
CHUNK, CHUNKS = 256, 4
HALF = CHUNK // 2
EPS = 1e-06
VMEM_ALL = 67_043_328


def kernel(
    tok, gain_in, gw_in, uw_in, dw_in,
    go, uo, do, mo,
    gt, ut, df, out, gain, gw, uw, dw, xs, sg, sud, dsend, tmp, xn, hid, part, far, near, comb, sums,
    ps, pr, gxs, gxr, gzs, gzr, us, ur, uxs, uxr, ufs, ufr, ds_, dr, ts, tr, tfs, tfr, rs, rr, loc,
):
    f, y = lax.axis_index("fs"), lax.axis_index("tp")
    z, x, c = f // 8, (f // 2) % 4, f % 2
    za, zb = z // 2, z % 2

    def at(zz, xx, cc, yy):
        return ((zz * NX + xx) * NC + cc, yy)

    zp, zm = (z + 1) % NZ, (z + 7) % NZ
    xp, xm, x2 = (x + 1) % NX, (x + 3) % NX, (x + 2) % NX
    yp, ym, y2 = (y + 1) % NY, (y + 3) % NY, (y + 2) % NY
    z_next, z_prev = at(zp, x, c, y), at(zm, x, c, y)
    x_next, x_prev, x_far = at(z, xp, c, y), at(z, xm, c, y), at(z, x2, c, y)
    y_next, y_prev = at(z, x, c, yp), at(z, x, c, ym)
    twin = at(z, x, 1 - c, y)
    pz = 2 * y + zb
    swap = at(pz, x, c, za)
    moves = za != y

    def remote(src, dst, send, recv, device):
        return pltpu.make_async_remote_copy(
            src_ref=src, dst_ref=dst, send_sem=send, recv_sem=recv, device_id=device, device_id_type=MESH
        )

    own_tokens = pltpu.make_async_copy(tok, xs.at[y], loc.at[0])
    own = [
        pltpu.make_async_copy(src, dst, loc.at[1 + n])
        for n, (src, dst) in enumerate(((gain_in, gain), (gw_in, gw), (uw_in, uw), (dw_in, dw)))
    ]
    for copy in own:
        copy.start()
    own_tokens.start()

    barrier = pltpu.get_barrier_semaphore()
    for partner in (z_next, z_prev, x_next, x_prev, x_far, y_next, y_prev, twin):
        pl.semaphore_signal(barrier, inc=1, device_id=partner, device_id_type=MESH)

    @pl.when(moves)
    def _():
        pl.semaphore_signal(barrier, inc=1, device_id=swap, device_id_type=MESH)

    for copy in own:
        copy.wait()

    eye = lax.broadcasted_iota(jnp.int32, (ROWS, ROWS), 0) == lax.broadcasted_iota(jnp.int32, (ROWS, ROWS), 1)
    scale = jnp.sum(jnp.where(eye, jnp.broadcast_to(gain[...], (ROWS, ROWS)), 0.0), axis=1, keepdims=True)
    tail = jnp.zeros((ROWS, WIDE - HID), F32)
    sg[z, x, c] = jnp.concatenate([scale * gw[...], tail], axis=1).astype(BF)
    sud[z, x, c, 0] = jnp.concatenate([scale * uw[...], tail], axis=1).astype(BF)
    low = jnp.concatenate([dw[pl.ds(ROWS, DROWS - ROWS), :], jnp.zeros((4, COLS), F32)], axis=0)
    right = jnp.concatenate([low[:, :256], low[:, 256:]], axis=0)
    packed = jnp.concatenate([dw[pl.ds(0, ROWS), :], right], axis=1).astype(BF)

    @pl.when(moves)
    def _():
        dsend[...] = packed

    @pl.when(jnp.logical_not(moves))
    def _():
        sud[z, x, c, 1] = packed

    df[pl.ds(HID, WIDE - HID), :] = jnp.zeros((WIDE - HID, D), BF)

    with jax.named_scope("meet"):
        pl.semaphore_wait(barrier, 8 + moves.astype(jnp.int32))

    sends = []

    def go_(copy):
        copy.start()
        sends.append(copy)

    change = remote(dsend, sud.at[pz, x, c, 1], ps.at[0], pr.at[0], swap)

    @pl.when(moves)
    def _():
        change.start()

    def token_copy(way, j):
        rows = pl.ds(j * CHUNK, CHUNK)
        return remote(
            tok.at[rows], xs.at[y, rows], ts.at[way * CHUNKS + j], tr.at[way * CHUNKS + j], (y_next, y_prev)[way]
        )

    def token_forward(way, j):
        rows = pl.ds(j * CHUNK + way * HALF, HALF)
        block = xs.at[(ym, yp)[way], rows]
        return remote(block, block, tfs.at[way * CHUNKS + j], tfr.at[way * CHUNKS + j], (y_next, y_prev)[way])

    def token_pass(j):
        for way in range(2):
            token_copy(way, j).wait_recv()
            go_(token_forward(way, j))

    order = [0, 7, 1, 6, 2, 5, 3, 4]
    turn = [0, 0, 1, 0, 1, 0, 1, 1]
    last = (4, 3)

    def came(way, k):
        return (z + (NZ - k if way == 0 else k)) % NZ

    def place(way, k):
        return 7 if k == 4 else 2 * k - 1 + way

    def ud_z(q, way, k):
        block, n = sud.at[came(way, k), x, c, q], (q * 2 + way) * 4 + k
        return remote(block, block, us.at[n], ur.at[n], (z_next, z_prev)[way])

    def ud_x(q, o, way):
        block, n = sud.at[(z + order[o]) % NZ, x, c, q], (q * 8 + o) * 2 + way
        return remote(block, block, uxs.at[n], uxr.at[n], (x_next, x_prev)[way])

    def ud_f(q, o):
        way, n = turn[o], q * 8 + o
        block = sud.at[(z + order[o]) % NZ, (xm, xp)[way], c, q]
        return remote(block, block, ufs.at[n], ufr.at[n], (x_next, x_prev)[way])

    def g_z(way, k, e):
        block, n = sg.at[came(way, k), (x, xp, xm, x2)[e], c], (way * 4 + k) * 4 + e
        return remote(block, block, gzs.at[n], gzr.at[n], (z_next, z_prev)[way])

    def twin_copy(n, block):
        return remote(block, block, ds_.at[n], dr.at[n], twin)

    def g_twin(o, cc):
        return twin_copy(o, sg.at[(z + order[o]) % NZ, :, cc])

    def ud_twin(o, cc):
        return twin_copy(8 + o, sud.at[(z + order[o]) % NZ, :, cc])

    def ud_arrived(q, o):
        for way in range(2):
            go_(ud_x(q, o, way))

    def ud_round(q, k):
        for way in range(2):
            if k <= last[way]:
                ud_z(q, way, k - 1).wait_recv()
                if k < last[way]:
                    go_(ud_z(q, way, k))
                ud_arrived(q, place(way, k))

    def g_round(k, es):
        for e in es:
            for way in range(2):
                if k <= last[way]:
                    g_z(way, k - 1, e).wait_recv()
                    if k < last[way]:
                        go_(g_z(way, k, e))
        if es[-1] == 3:
            for way in range(2):
                if k <= last[way]:
                    go_(g_twin(place(way, k), c))

    def x_pass(*os):
        for o in os:
            for q in range(2):
                for way in range(2):
                    ud_x(q, o, way).wait_recv()
                go_(ud_f(q, o))

    def x_end(*os):
        for o in os:
            for q in range(2):
                ud_f(q, o).wait_recv()
            go_(ud_twin(o, c))

    own_gate = sg.at[z, x, c]
    gx = [remote(own_gate, own_gate, gxs.at[k], gxr.at[k], to) for k, to in enumerate((x_next, x_prev, x_far))]
    for way in range(2):
        go_(ud_z(0, way, 0))
    for copy in gx:
        go_(copy)
    for way in range(2):
        go_(g_z(way, 0, 0))
    ud_arrived(0, 0)
    for j in range(CHUNKS):
        for way in range(2):
            go_(token_copy(way, j))

    with jax.named_scope("change"):

        @pl.when(moves)
        def _():
            change.wait_recv()

    for way in range(2):
        go_(ud_z(1, way, 0))
    ud_arrived(1, 0)
    with jax.named_scope("gate_x"):
        for copy in gx:
            copy.wait_recv()
    for way in range(2):
        go_(g_z(way, 0, 1))
    go_(g_twin(0, c))

    with jax.named_scope("round_1"):
        ud_round(0, 1)
        ud_round(1, 1)
        for e in (2, 3):
            for way in range(2):
                go_(g_z(way, 0, e))
        x_pass(0)
    with jax.named_scope("round_2"):
        ud_round(0, 2)
        ud_round(1, 2)
        g_round(1, (0, 1))
        x_pass(1, 2)
        x_end(0)
        token_pass(0)
    with jax.named_scope("round_3"):
        ud_round(0, 3)
        ud_round(1, 3)
        g_round(1, (2, 3))
        x_pass(3, 4)
        x_end(1, 2)
    with jax.named_scope("round_4"):
        ud_round(0, 4)
        ud_round(1, 4)
        g_round(2, (0, 1))
        token_pass(1)
        x_pass(5, 6)
        x_end(3, 4)
    with jax.named_scope("round_5"):
        g_round(2, (2, 3))
        token_pass(2)
        x_pass(7)
    with jax.named_scope("round_6"):
        g_round(3, (0, 1, 2, 3))
        x_end(5, 6)
        token_pass(3)
    with jax.named_scope("round_7"):
        x_end(7)
        g_round(4, (0, 1, 2, 3))
    with jax.named_scope("tail_twin"):
        for o in range(8):
            g_twin(o, 1 - c).wait_recv()
            ud_twin(o, 1 - c).wait_recv()

    def assemble(n, carry):
        a, group = n // 4, n % 4
        for s in range(4):
            shard = sud[2 * a + group // 2, (group % 2) * 2 + s // 2, s % 2, 1].astype(F32)
            tmp[pl.ds(DROWS * s, ROWS), :] = shard[:, :COLS]
            at_row = DROWS * s + ROWS
            tmp[pl.ds(at_row, DROWS - ROWS), pl.ds(0, 256)] = shard[: DROWS - ROWS, COLS:]
            tmp[pl.ds(at_row, DROWS - ROWS), pl.ds(256, 256)] = shard[16 : 16 + DROWS - ROWS, COLS:]
        rows = pl.ds(pl.multiple_of(group * 176, 16), 176)
        df[rows, pl.ds(pl.multiple_of(a * COLS, COLS), COLS)] = tmp[...].astype(BF)
        return carry

    with jax.named_scope("assemble"):
        lax.fori_loop(0, 16, assemble, 0)
    own_tokens.wait()

    def message(kind, way, j):
        rows = {"far": 1 - way, "near": way, "comb": 1 - way}[kind]
        to_block = y2 if kind == "far" else (yp, ym)[way]
        src = sums.at[way, j] if kind == "comb" else part.at[j, to_block, pl.ds(rows * HALF, HALF)]
        dst = {"far": far, "near": near, "comb": comb}[kind].at[way, j]
        n = (("far", "near", "comb").index(kind) * 2 + way) * CHUNKS + j
        return remote(src, dst, rs.at[n], rr.at[n], (y_next, y_prev)[way])

    def compute(j):
        with jax.named_scope("wait_tokens"):
            for way in range(2):
                token_forward(way, j).wait_recv()

        def normalise(t, carry):
            rows = pl.ds(pl.multiple_of(j * CHUNK + t * 32, 32), 32)
            total = jnp.zeros((32, 1), F32)
            for b in range(NY):
                v = xs[b, rows, :].astype(F32)
                total = total + jnp.sum(v * v, axis=1, keepdims=True)
            r = lax.rsqrt(total / D + EPS)
            for b in range(NY):
                v = xs[b, rows, :].astype(F32)
                xn[pl.ds(pl.multiple_of(t * 32, 32), 32), pl.ds(b * COLS, COLS)] = (v * r).astype(BF)
            return carry

        with jax.named_scope("normalise"):
            lax.fori_loop(0, CHUNK // 32, normalise, 0)

        def first(n, carry):
            cols = pl.ds(pl.multiple_of(n * 256, 256), 256)
            gate = jnp.dot(xn[...], sg[:, :, :, :, cols].reshape(D, 256), preferred_element_type=F32)
            up = jnp.dot(xn[...], sud[:, :, :, 0, :, cols].reshape(D, 256), preferred_element_type=F32)
            hid[:, cols] = (gate / (1.0 + jnp.exp(-gate)) * up).astype(BF)
            return carry

        with jax.named_scope("first"):
            lax.fori_loop(0, WIDE // 256, first, 0)

        def second(n, carry):
            b = (y + 2 + n) % NY
            cols = pl.ds(pl.multiple_of(b * COLS, COLS), COLS)
            part[j, b] = jnp.dot(hid[...], df[:, cols], preferred_element_type=F32).astype(BF)
            return carry

        with jax.named_scope("second"):
            lax.fori_loop(0, NY, second, 0)
        for kind in ("far", "near"):
            for way in range(2):
                message(kind, way, j).start()

    def combine(j):
        for way in range(2):
            message("far", way, j).wait_recv()
            rows = pl.ds((1 - way) * HALF, HALF)
            mine = part[j, (yp, ym)[way], rows, :].astype(F32)
            sums[way, j] = (mine + far[way, j].astype(F32)).astype(BF)
        for way in range(2):
            message("comb", way, j).start()

    def step(j, carry):
        @pl.when(j < CHUNKS)
        def _():
            with jax.named_scope("compute"):
                compute(j)

        @pl.when(j > 0)
        def _():
            with jax.named_scope("combine"):
                combine(j - 1)

        return carry

    lax.fori_loop(0, CHUNKS + 1, step, 0)

    one = lax.broadcasted_iota(jnp.int32, (256, 256), 0) == lax.broadcasted_iota(jnp.int32, (256, 256), 1)
    unit = one.astype(F32).astype(BF)

    def turn_over(n, carry):
        q, cols = n % 4, pl.ds(pl.multiple_of(n // 4 * 256, 256), 256)
        to = pl.ds(pl.multiple_of(q * 512, 512), 512)
        for dst, src in ((gt, sg[pl.ds(2 * q, 2), :, :, :, cols]), (ut, sud[pl.ds(2 * q, 2), :, :, 0, :, cols])):
            dst[cols, to] = lax.dot_general(
                unit, src.reshape(512, 256), (((1,), (1,)), ((), ())), preferred_element_type=F32
            ).astype(BF)
        return carry

    with jax.named_scope("turn_over"):
        lax.fori_loop(0, 12, turn_over, 0)
    leaving = [
        pltpu.make_async_copy(src.at[pl.ds(0, HID)], dst, loc.at[5 + n])
        for n, (src, dst) in enumerate(((gt, go), (ut, uo), (df, do)))
    ]
    for copy in leaving:
        copy.start()

    def out_copy(j):
        rows = pl.ds(pl.multiple_of(j * CHUNK, CHUNK), CHUNK)
        return pltpu.make_async_copy(out.at[rows], mo.at[rows], loc.at[8 + j])

    def finish(j, carry):
        for way in range(2):
            message("near", way, j).wait_recv()
            message("comb", way, j).wait_recv()
        for half in range(2):
            rows = pl.ds(half * HALF, HALF)
            mine = part[j, y, rows, :].astype(F32)
            total = mine + near[half, j].astype(F32) + comb[1 - half, j].astype(F32)
            out[pl.ds(pl.multiple_of(j * CHUNK + half * HALF, HALF), HALF), :] = total.astype(BF)
        out_copy(j).start()
        return carry

    with jax.named_scope("finish"):
        lax.fori_loop(0, CHUNKS, finish, 0)

    for copy in sends:
        copy.wait_send()

    @pl.when(moves)
    def _():
        change.wait_send()

    def drain(j, carry):
        for kind in ("far", "near", "comb"):
            for way in range(2):
                message(kind, way, j).wait_send()
        out_copy(j).wait()
        return carry

    with jax.named_scope("drain"):
        lax.fori_loop(0, CHUNKS, drain, 0)
        for copy in leaving:
            copy.wait()


def hand_out(gt, ut, df, out, go, uo, do, mo, held, sem):
    n = 0
    moves = []
    for src, dst, rows in ((out, mo, 256), (gt, go, 176), (ut, uo, 176), (df, do, 176)):
        for k in range(4):
            part = pl.ds(k * rows, rows)
            slot = held.at[n, pl.ds(0, rows), pl.ds(0, src.shape[1])]
            moves.append(
                (
                    pltpu.make_async_copy(src.at[part], slot, sem.at[0, n]),
                    pltpu.make_async_copy(slot, dst.at[part], sem.at[1, n]),
                )
            )
            n += 1
    for come, _ in moves:
        come.start()
    for come, leave in moves:
        come.wait()
        leave.start()
    for _, leave in moves:
        leave.wait()


def shards(tokens, norm_gain, gate_weight, up_weight, down_weight):
    vmem = functools.partial(pltpu.VMEM, dtype=BF)
    sem = pltpu.SemaphoreType.DMA
    hbm = pl.BlockSpec(memory_space=pltpu.HBM)
    held = pl.pallas_call(
        kernel,
        name="layer",
        out_shape=(jax.ShapeDtypeStruct((HID, D), BF),) * 3 + (jax.ShapeDtypeStruct((CHUNK * CHUNKS, COLS), BF),),
        in_specs=[hbm] * 5,
        out_specs=(hbm,) * 4,
        scratch_shapes=[
            vmem((WIDE, D)),
            vmem((WIDE, D)),
            vmem((WIDE, D)),
            vmem((CHUNK * CHUNKS, COLS)),
            pltpu.VMEM((1, ROWS), F32),
            pltpu.VMEM((ROWS, HID), F32),
            pltpu.VMEM((ROWS, HID), F32),
            pltpu.VMEM((DROWS, COLS), F32),
            vmem((NY, CHUNK * CHUNKS, COLS)),
            vmem((NZ, NX, NC, ROWS, WIDE)),
            vmem((NZ, NX, NC, 2, ROWS, WIDE)),
            vmem((ROWS, WIDE)),
            pltpu.VMEM((4 * DROWS, COLS), F32),
            vmem((CHUNK, D)),
            vmem((CHUNK, WIDE)),
            vmem((CHUNKS, NY, CHUNK, COLS)),
            vmem((2, CHUNKS, HALF, COLS)),
            vmem((2, CHUNKS, HALF, COLS)),
            vmem((2, CHUNKS, HALF, COLS)),
            vmem((2, CHUNKS, HALF, COLS)),
            sem((1,)), sem((1,)),
            sem((3,)), sem((3,)),
            sem((32,)), sem((32,)),
            sem((16,)), sem((16,)),
            sem((32,)), sem((32,)),
            sem((16,)), sem((16,)),
            sem((16,)), sem((16,)),
            sem((8,)), sem((8,)),
            sem((8,)), sem((8,)),
            sem((24,)), sem((24,)),
            sem((12,)),
        ],
        compiler_params=pltpu.CompilerParams(collective_id=0, has_side_effects=True, vmem_limit_bytes=VMEM_ALL),
    )(tokens, norm_gain.reshape(1, ROWS), gate_weight, up_weight, down_weight)
    gate, up, down, mixed = pl.pallas_call(
        hand_out,
        name="hand_out",
        out_shape=(jax.ShapeDtypeStruct((HID, D), BF),) * 3 + (jax.ShapeDtypeStruct((CHUNK * CHUNKS, COLS), BF),),
        in_specs=[hbm] * 4,
        out_specs=(hbm,) * 4,
        scratch_shapes=[vmem((16, CHUNK, D)), sem((2, 16))],
        compiler_params=pltpu.CompilerParams(vmem_limit_bytes=VMEM_ALL),
    )(*held)
    return (gate.T, up.T, down, mixed)


def solution(mesh):
    return jax.shard_map(
        shards,
        mesh=mesh,
        in_specs=(P("fs", "tp"), P("fs"), P("fs", "tp"), P("fs", "tp"), P("fs", "tp")),
        out_specs=(P(None, "tp"), P(None, "tp"), P("tp", None), P("fs", "tp")),
        check_vma=False,
    )
```

```python
import functools

import jax
import jax.numpy as jnp
from jax import lax
from jax.experimental import pallas as pl
from jax.experimental.pallas import tpu as pltpu
from jax.sharding import PartitionSpec as P

MESH = pl.DeviceIdType.MESH
BF = jnp.bfloat16
F32 = jnp.float32
NZ, NX, NC, NY = 8, 4, 2, 4
ROWS = 32
HID = 704
WIDE = 768
DROWS, COLS = 44, 512
D = 2048
CHUNK, CHUNKS = 128, 8
PIECE, PIECES = 256, 4
HALF = CHUNK // 2
EPS = 1e-06
LIMIT = 38 * 2**20


def kernel(
    tok, gw, uw, dw,
    gt, ut, df, out,
    xs, sg, sud, dsend, tmp, xn, hid, part, far, got, sums,
    ps, pr, gxs, gxr, gzs, gzr, us, ur, uxs, uxr, ufs, ufr, ds_, dr, ts, tr, tfs, tfr, rs, rr, loc,
):
    f, y = lax.axis_index("fs"), lax.axis_index("tp")
    z, x, c = f // 8, (f // 2) % 4, f % 2
    za, zb = z // 2, z % 2

    def at(zz, xx, cc, yy):
        return ((zz * NX + xx) * NC + cc, yy)

    zp, zm = (z + 1) % NZ, (z + 7) % NZ
    xp, xm, x2 = (x + 1) % NX, (x + 3) % NX, (x + 2) % NX
    yp, ym, y2 = (y + 1) % NY, (y + 3) % NY, (y + 2) % NY
    z_next, z_prev = at(zp, x, c, y), at(zm, x, c, y)
    x_next, x_prev, x_far = at(z, xp, c, y), at(z, xm, c, y), at(z, x2, c, y)
    y_next, y_prev = at(z, x, c, yp), at(z, x, c, ym)
    twin = at(z, x, 1 - c, y)
    pz = 2 * y + zb
    swap = at(pz, x, c, za)
    moves = za != y

    def remote(src, dst, send, recv, device):
        return pltpu.make_async_remote_copy(
            src_ref=src, dst_ref=dst, send_sem=send, recv_sem=recv, device_id=device, device_id_type=MESH
        )

    own_tokens = pltpu.make_async_copy(tok, xs.at[y], loc.at[0])

    barrier = pltpu.get_barrier_semaphore()
    for partner in (z_next, z_prev, x_next, x_prev, x_far, y_next, y_prev, twin):
        pl.semaphore_signal(barrier, inc=1, device_id=partner, device_id_type=MESH)

    @pl.when(moves)
    def _():
        pl.semaphore_signal(barrier, inc=1, device_id=swap, device_id_type=MESH)

    with jax.named_scope("meet"):
        pl.semaphore_wait(barrier, 8 + moves.astype(jnp.int32))

    def token_copy(way, j):
        rows = pl.ds(j * PIECE, PIECE)
        return remote(tok.at[rows], xs.at[y, rows], ts.at[way], tr.at[way * PIECES + j], (y_next, y_prev)[way])

    def token_forward(way, j):
        rows = pl.ds(j * PIECE + way * (PIECE // 2), PIECE // 2)
        block = xs.at[(ym, yp)[way], rows]
        return remote(block, block, tfs.at[way], tfr.at[way * PIECES + j], (y_next, y_prev)[way])

    def token_pass(j):
        for way in range(2):
            token_copy(way, j).wait_recv()
            token_forward(way, j).start()

    for j in range(PIECES):
        for way in range(2):
            token_copy(way, j).start()
    own_tokens.start()

    head = dw[pl.ds(0, ROWS), :]
    low = jnp.concatenate([dw[pl.ds(ROWS, DROWS - ROWS), :].astype(F32), jnp.zeros((4, COLS), F32)], axis=0)
    right = jnp.concatenate([low[:, : COLS // 2], low[:, COLS // 2 :]], axis=0).astype(BF)

    @pl.when(moves)
    def _():
        dsend[:, pl.ds(0, COLS)] = head
        dsend[:, pl.ds(COLS, COLS // 2)] = right

    @pl.when(jnp.logical_not(moves))
    def _():
        sud[z, x, c, 1, :, pl.ds(0, COLS)] = head
        sud[z, x, c, 1, :, pl.ds(COLS, COLS // 2)] = right

    tail = jnp.zeros((ROWS, WIDE - HID), BF)
    sud[z, x, c, 0] = jnp.concatenate([uw[...], tail], axis=1)
    sg[z, x, c] = jnp.concatenate([gw[...], tail], axis=1)

    change = remote(dsend, sud.at[pz, x, c, 1], ps.at[0], pr.at[0], swap)

    @pl.when(moves)
    def _():
        change.start()

    order = [0, 7, 1, 6, 2, 5, 3, 4]
    last = (4, 3)

    def came(way, k):
        return (z + (NZ - k if way == 0 else k)) % NZ

    def place(way, k):
        return 7 if k == 4 else 2 * k - 1 + way

    def ud_z(q, way, k):
        block = sud.at[came(way, k), x, c, q]
        return remote(block, block, us.at[way], ur.at[(q * 2 + way) * 4 + k], (z_next, z_prev)[way])

    def ud_x(q, o, way):
        block = sud.at[(z + order[o]) % NZ, x, c, q]
        return remote(block, block, uxs.at[0], uxr.at[(q * 8 + o) * 2 + way], (x_next, x_prev)[way])

    def ud_f(q, o):
        block = sud.at[(z + order[o]) % NZ, (xm, xp)[q], c, q]
        return remote(block, block, ufs.at[0], ufr.at[q * 8 + o], (x_next, x_prev)[q])

    def g_z(way, k, e):
        block = sg.at[came(way, k), (x, xp, xm, x2)[e], c]
        return remote(block, block, gzs.at[way], gzr.at[(way * 4 + k) * 2 + e // 2], (z_next, z_prev)[way])

    def g_pair(way, k, h):
        block = sg.at[came(way, k), pl.ds(0, 2), c]
        return remote(block, block, gzs.at[way], gzr.at[(way * 4 + k) * 2 + h], (z_next, z_prev)[way])

    def g_twin(o):
        block = sg.at[(z + order[o]) % NZ, :, c]
        return remote(block, block, ds_.at[2], dr.at[2], twin)

    def ud_twin(q, o):
        block = sud.at[(z + order[o]) % NZ, :, c, q]
        return remote(block, block, ds_.at[q], dr.at[q], twin)

    def twins(n):
        block = sg.at[:, :, c] if n == 2 else sud.at[:, :, c, n]
        return remote(block, block, ds_.at[n], dr.at[n], twin)

    def ud_arrived(q, o):
        for way in range(2):
            ud_x(q, o, way).start()

    def ud_round(q, k):
        for way in range(2):
            if k <= last[way]:
                ud_z(q, way, k - 1).wait_recv()
                if k < last[way]:
                    ud_z(q, way, k).start()
                ud_arrived(q, place(way, k))

    def g_round(k, *hs):
        for h in hs:
            for way in range(2):
                if k <= last[way]:
                    g_pair(way, k - 1, h).wait_recv()
                    if k < last[way]:
                        for e in (2 * h, 2 * h + 1):
                            g_z(way, k, e).start()
                    if h == 1:
                        g_twin(place(way, k)).start()

    def x_pass(q, *os):
        for o in os:
            for way in (q, 1 - q):
                ud_x(q, o, way).wait_recv()
                if way == q:
                    ud_f(q, o).start()

    def x_end(q, *os):
        for o in os:
            ud_f(q, o).wait_recv()
            ud_twin(q, o).start()

    def g_x(k):
        block = sg.at[z, x, c]
        return remote(block, block, gxs.at[0], gxr.at[0], (x_next, x_prev, x_far)[k])

    three = sg.at[pl.ds(0, 3), x, c]
    all_gx = remote(three, three, gxs.at[0], gxr.at[0], x_next)

    for way in range(2):
        ud_z(0, way, 0).start()
    for k in range(3):
        g_x(k).start()
    ud_arrived(0, 0)
    for way in range(2):
        g_z(way, 0, 0).start()

    with jax.named_scope("change"):

        @pl.when(moves)
        def _():
            change.wait_recv()

    for way in range(2):
        ud_z(1, way, 0).start()
    ud_arrived(1, 0)
    with jax.named_scope("round_1"):
        ud_round(0, 1)
        all_gx.wait_recv()
        for e in (1, 2, 3):
            for way in range(2):
                g_z(way, 0, e).start()
        g_twin(0).start()
        x_pass(0, 0)
    with jax.named_scope("round_2"):
        ud_round(0, 2)
        ud_round(1, 1)
        x_pass(0, 1, 2)
        x_pass(1, 0)
        g_round(1, 0)
        x_end(0, 0)
        token_pass(0)
    with jax.named_scope("round_3"):
        ud_round(0, 3)
        ud_round(1, 2)
        x_pass(0, 3, 4)
        g_round(1, 1)
        x_pass(1, 1, 2)
        x_end(0, 1, 2)
        x_end(1, 0)
    with jax.named_scope("round_4"):
        ud_round(0, 4)
        ud_round(1, 3)
        x_pass(0, 5, 6)
        g_round(2, 0)
        token_pass(1)
        x_pass(1, 3, 4)
        x_end(0, 3, 4)
        x_end(1, 1, 2)
    with jax.named_scope("round_5"):
        ud_round(1, 4)
        x_pass(0, 7)
        g_round(2, 1)
        token_pass(2)
        x_pass(1, 5, 6)
        x_end(0, 5, 6)
        x_end(1, 3, 4)
    with jax.named_scope("round_6"):
        g_round(3, 0, 1)
        x_end(0, 7)
        x_pass(1, 7)
        token_pass(3)
    with jax.named_scope("round_7"):
        g_round(4, 0, 1)
        x_end(1, 5, 6)
    own_tokens.wait()

    def normalise(j):
        for k in range(PIECES):

            @pl.when(j == k * (PIECE // CHUNK))
            def _(k=k):
                for way in range(2):
                    token_forward(way, k).wait_recv()

        def rows_of(t, carry):
            rows = pl.ds(pl.multiple_of(j * CHUNK + t * 32, 32), 32)
            total = jnp.zeros((32, 1), F32)
            for b in range(NY):
                v = xs[b, rows, :].astype(F32)
                total = total + jnp.sum(v * v, axis=1, keepdims=True)
            r = lax.rsqrt(total / D + EPS)
            for b in range(NY):
                v = xs[b, rows, :].astype(F32)
                xn[pl.ds(pl.multiple_of(t * 32, 32), 32), pl.ds(b * COLS, COLS)] = (v * r).astype(BF)
            return carry

        lax.fori_loop(0, CHUNK // 32, rows_of, 0)

    def first():
        def columns(n, carry):
            cols = pl.ds(pl.multiple_of(n * 256, 256), 256)
            gate = jnp.dot(xn[...], sg[:, :, :, :, cols].reshape(D, 256), preferred_element_type=F32)
            up = jnp.dot(xn[...], sud[:, :, :, 0, :, cols].reshape(D, 256), preferred_element_type=F32)
            hid[:, cols] = (gate / (1.0 + jnp.exp(-gate)) * up).astype(BF)
            return carry

        lax.fori_loop(0, WIDE // 256, columns, 0)

    def message(kind, way, j):
        rows = {"far": 1 - way, "near": way, "comb": 1 - way}[kind]
        to_block = y2 if kind == "far" else (yp, ym)[way]
        src = sums.at[j, way] if kind == "comb" else part.at[j, to_block, pl.ds(rows * HALF, HALF)]
        dst = {"far": far.at[j, way], "near": got.at[j, way], "comb": got.at[j, 2 + way]}[kind]
        return remote(src, dst, rs.at[0], rr.at[j + (0 if kind == "far" else CHUNKS)], (y_next, y_prev)[way])

    def all_far(j):
        return remote(sums.at[j], far.at[j], rs.at[0], rr.at[j], y_next)

    def all_got(j):
        return remote(got.at[j], got.at[j], rs.at[0], rr.at[CHUNKS + j], y_next)

    def second(j):
        def block(n, carry):
            b = (y + 2 + n) % NY
            cols = pl.ds(pl.multiple_of(b * COLS, COLS), COLS)
            part[j, b] = jnp.dot(hid[...], df[:, cols], preferred_element_type=F32).astype(BF)

            @pl.when(n == 0)
            def _():
                for way in range(2):
                    message("far", way, j).start()

            return carry

        lax.fori_loop(0, NY, block, 0)
        for way in range(2):
            message("near", way, j).start()

    def combine(j):
        all_far(j).wait_recv()
        for way in range(2):
            mine = part[j, (yp, ym)[way], pl.ds((1 - way) * HALF, HALF), :].astype(F32)
            sums[j, way] = (mine + far[j, way].astype(F32)).astype(BF)
        for way in range(2):
            message("comb", way, j).start()

    with jax.named_scope("normalise_0"):
        normalise(0)
    with jax.named_scope("wait_up"):
        x_end(1, 7)
        twins(2).wait_recv()
        twins(0).wait_recv()
    with jax.named_scope("first_0"):
        first()
    with jax.named_scope("wait_down"):
        twins(1).wait_recv()

    def assemble(n, carry):
        a, group = n // 4, n % 4
        for s in range(4):
            shard = sud[2 * a + group // 2, (group % 2) * 2 + s // 2, s % 2, 1].astype(F32)
            tmp[pl.ds(DROWS * s, ROWS), :] = shard[:, :COLS]
            at_row = DROWS * s + ROWS
            tmp[pl.ds(at_row, DROWS - ROWS), pl.ds(0, 256)] = shard[: DROWS - ROWS, COLS:]
            tmp[pl.ds(at_row, DROWS - ROWS), pl.ds(256, 256)] = shard[16 : 16 + DROWS - ROWS, COLS:]
        rows = pl.ds(pl.multiple_of(group * 176, 16), 176)
        df[rows, pl.ds(pl.multiple_of(a * COLS, COLS), COLS)] = tmp[...].astype(BF)
        return carry

    with jax.named_scope("assemble"):
        df[pl.ds(HID, WIDE - HID), :] = jnp.zeros((WIDE - HID, D), BF)
        lax.fori_loop(0, 16, assemble, 0)

    one = lax.broadcasted_iota(jnp.int32, (256, 256), 0) == lax.broadcasted_iota(jnp.int32, (256, 256), 1)
    unit = one.astype(F32).astype(BF)

    def turn_over(n, carry):
        q, cols = n % 4, pl.ds(pl.multiple_of(n // 4 * 256, 256), 256)
        to = pl.ds(pl.multiple_of(q * 512, 512), 512)
        for dst, src in ((gt, sg[pl.ds(2 * q, 2), :, :, :, cols]), (ut, sud[pl.ds(2 * q, 2), :, :, 0, :, cols])):
            dst[cols, to] = lax.dot_general(
                unit, src.reshape(512, 256), (((1,), (1,)), ((), ())), preferred_element_type=F32
            ).astype(BF)
        return carry

    def step(j, carry):
        @pl.when(j < CHUNKS)
        def _():
            with jax.named_scope("second"):
                second(j)

        @pl.when(j > 0)
        def _():
            with jax.named_scope("combine"):
                combine(j - 1)

        @pl.when(j < CHUNKS - 1)
        def _():
            with jax.named_scope("first"):
                normalise(j + 1)
                first()

        @pl.when(jnp.logical_and(j >= 3, j < 7))
        def _():
            with jax.named_scope("turn_over"):
                lax.fori_loop(3 * j - 9, 3 * j - 6, turn_over, 0)

        return carry

    lax.fori_loop(0, CHUNKS + 1, step, 0)

    def finish(j, carry):
        all_got(j).wait_recv()
        for half in range(2):
            mine = part[j, y, pl.ds(half * HALF, HALF), :].astype(F32)
            total = mine + got[j, half].astype(F32) + got[j, 3 - half].astype(F32)
            out[pl.ds(pl.multiple_of(j * CHUNK + half * HALF, HALF), HALF), :] = total.astype(BF)
        return carry

    with jax.named_scope("finish"):
        lax.fori_loop(0, CHUNKS, finish, 0)

    with jax.named_scope("drain"):

        @pl.when(moves)
        def _():
            change.wait_send()

        all_gx.wait_send()
        for way, n in ((0, 4), (1, 3)):
            eight = sg.at[pl.ds(0, n), x]
            remote(eight, eight, us.at[way], ur.at[0], z_next).wait_send()
            four = sg.at[pl.ds(0, n), :, c]
            remote(four, four, gzs.at[way], gzr.at[0], z_next).wait_send()
            remote(tok, xs.at[y], ts.at[way], tr.at[0], y_next).wait_send()
            half = xs.at[0, pl.ds(0, PIECE * PIECES // 2)]
            remote(half, half, tfs.at[way], tfr.at[0], y_next).wait_send()
        block = sg.at[:, :, c]
        remote(block, block, uxs.at[0], uxr.at[0], x_next).wait_send()
        block = sg.at[pl.ds(0, 4), :, c]
        remote(block, block, ufs.at[0], ufr.at[0], x_next).wait_send()
        for n in range(3):
            twins(n).wait_send()
        block = xs.at[pl.ds(0, 3)]
        remote(block, block, rs.at[0], rr.at[0], y_next).wait_send()


def hand_out(gt, ut, df, out, go, uo, do, mo, sem):
    rows = pl.ds(0, HID)
    moved = ((gt.at[rows], go), (ut.at[rows], uo), (df.at[rows], do), (out, mo))
    copies = [pltpu.make_async_copy(src, dst, sem.at[n]) for n, (src, dst) in enumerate(moved)]
    for copy in copies:
        copy.start()
    for copy in copies:
        copy.wait()


def shards(tokens, norm_gain, gate_weight, up_weight, down_weight):
    vmem = functools.partial(pltpu.VMEM, dtype=BF)
    sem = pltpu.SemaphoreType.DMA
    hbm = pl.BlockSpec(memory_space=pltpu.HBM)
    held = pl.pallas_call(
        kernel,
        name="layer",
        out_shape=(jax.ShapeDtypeStruct((WIDE, D), BF),) * 3 + (jax.ShapeDtypeStruct((CHUNK * CHUNKS, COLS), BF),),
        in_specs=[hbm] + [pl.BlockSpec(memory_space=pltpu.VMEM)] * 3,
        out_specs=(pl.BlockSpec(memory_space=pltpu.VMEM),) * 4,
        scratch_shapes=[
            vmem((NY, CHUNK * CHUNKS, COLS)),
            vmem((NZ, NX, NC, ROWS, WIDE)),
            vmem((NZ, NX, NC, 2, ROWS, WIDE)),
            vmem((ROWS, WIDE)),
            pltpu.VMEM((4 * DROWS, COLS), F32),
            vmem((CHUNK, D)),
            vmem((CHUNK, WIDE)),
            vmem((CHUNKS, NY, CHUNK, COLS)),
            vmem((CHUNKS, 2, HALF, COLS)),
            vmem((CHUNKS, 4, HALF, COLS)),
            vmem((CHUNKS, 2, HALF, COLS)),
            sem((1,)), sem((1,)),
            sem((1,)), sem((1,)),
            sem((2,)), sem((16,)),
            sem((2,)), sem((16,)),
            sem((1,)), sem((32,)),
            sem((1,)), sem((16,)),
            sem((3,)), sem((3,)),
            sem((2,)), sem((2 * PIECES,)),
            sem((2,)), sem((2 * PIECES,)),
            sem((1,)), sem((2 * CHUNKS,)),
            sem((1,)),
        ],
        compiler_params=pltpu.CompilerParams(collective_id=0, has_side_effects=True, vmem_limit_bytes=LIMIT),
    )(
        tokens,
        (norm_gain[:, None] * gate_weight).astype(BF),
        (norm_gain[:, None] * up_weight).astype(BF),
        down_weight.astype(BF),
    )
    gate, up, down, mixed = pl.pallas_call(
        hand_out,
        name="hand_out",
        out_shape=(jax.ShapeDtypeStruct((HID, D), BF),) * 3 + (jax.ShapeDtypeStruct((CHUNK * CHUNKS, COLS), BF),),
        in_specs=[pl.BlockSpec(memory_space=pl.ANY)] * 4,
        out_specs=(hbm,) * 4,
        scratch_shapes=[sem((4,))],
        compiler_params=pltpu.CompilerParams(vmem_limit_bytes=2**20),
    )(*held)
    return (gate.T, up.T, down, mixed)


def solution(mesh):
    return jax.shard_map(
        shards,
        mesh=mesh,
        in_specs=(P("fs", "tp"), P("fs"), P("fs", "tp"), P("fs", "tp"), P("fs", "tp")),
        out_specs=(P(None, "tp"), P(None, "tp"), P("tp", None), P("fs", "tp")),
        check_vma=False,
    )
```

```python
import functools

import jax
import jax.numpy as jnp
from jax import lax
from jax.experimental import pallas as pl
from jax.experimental.pallas import tpu as pltpu
from jax.sharding import PartitionSpec as P

MESH = pl.DeviceIdType.MESH
BF = jnp.bfloat16
F32 = jnp.float32
NZ, NX, NC, NY = 8, 4, 2, 4
ROWS = 32
HID = 704
WIDE = 768
TILES = 11
DROWS, COLS = 44, 512
D = 2048
CHUNK, CHUNKS = 128, 8
PIECE, PIECES = 256, 4
HALF = CHUNK // 2
EPS = 1e-06
LIMIT = 38 * 2**20


def kernel(
    tok, gw, uw, dw,
    gt, ut, df, out,
    xs, sg, sud, ends, dsend, tmp, xn, hid, part, far, got, sums,
    ps, pr, gxs, gxr, gzs, gzr, us, ur, uxs, uxr, ufs, ufr, ds_, dr, ts, tr, tfs, tfr, rs, rr, loc,
):
    f, y = lax.axis_index("fs"), lax.axis_index("tp")
    z, x, c = f // 8, (f // 2) % 4, f % 2
    za, zb = z // 2, z % 2

    def at(zz, xx, cc, yy):
        return ((zz * NX + xx) * NC + cc, yy)

    zp, zm = (z + 1) % NZ, (z + 7) % NZ
    xp, xm, x2 = (x + 1) % NX, (x + 3) % NX, (x + 2) % NX
    yp, ym, y2 = (y + 1) % NY, (y + 3) % NY, (y + 2) % NY
    z_next, z_prev = at(zp, x, c, y), at(zm, x, c, y)
    x_next, x_prev, x_far = at(z, xp, c, y), at(z, xm, c, y), at(z, x2, c, y)
    y_next, y_prev = at(z, x, c, yp), at(z, x, c, ym)
    twin = at(z, x, 1 - c, y)
    pz = 2 * y + zb
    swap = at(pz, x, c, za)
    moves = za != y

    def remote(src, dst, send, recv, device):
        return pltpu.make_async_remote_copy(
            src_ref=src, dst_ref=dst, send_sem=send, recv_sem=recv, device_id=device, device_id_type=MESH
        )

    own_tokens = pltpu.make_async_copy(tok, xs.at[y], loc.at[0])

    barrier = pltpu.get_barrier_semaphore()
    for partner in (z_next, z_prev, x_next, x_prev, x_far, y_next, y_prev, twin):
        pl.semaphore_signal(barrier, inc=1, device_id=partner, device_id_type=MESH)

    @pl.when(moves)
    def _():
        pl.semaphore_signal(barrier, inc=1, device_id=swap, device_id_type=MESH)

    with jax.named_scope("meet"):
        pl.semaphore_wait(barrier, 8 + moves.astype(jnp.int32))

    def token_copy(way, j):
        rows = pl.ds(j * PIECE, PIECE)
        return remote(tok.at[rows], xs.at[y, rows], ts.at[way], tr.at[way * PIECES + j], (y_next, y_prev)[way])

    def token_forward(way, j):
        rows = pl.ds(j * PIECE + way * (PIECE // 2), PIECE // 2)
        block = xs.at[(ym, yp)[way], rows]
        return remote(block, block, tfs.at[way], tfr.at[way * PIECES + j], (y_next, y_prev)[way])

    def token_pass(j):
        for way in range(2):
            token_copy(way, j).wait_recv()
            token_forward(way, j).start()

    for j in range(PIECES):
        for way in range(2):
            token_copy(way, j).start()
    own_tokens.start()

    for ref, dst in ((uw, sud.at[z, x, c, 0]), (gw, sg.at[z, x, c])):
        for t in range(5):
            for r in range(2):
                dst[2 * t + r] = ref[pl.ds(16 * r, 16), pl.ds(128 * t, 128)]
        dst[10] = jnp.concatenate([ref[pl.ds(16 * r, 16), pl.ds(640, 64)] for r in range(2)], axis=1)

    def own_down(dst):
        for t in range(4):
            for r in range(2):
                dst[2 * t + r] = dw[pl.ds(16 * r, 16), pl.ds(128 * t, 128)]
        low = dw[pl.ds(ROWS, DROWS - ROWS), :].astype(F32)
        for p in range(3):
            piece = [low[:, 128 * p : 128 * p + 128], low[4 * p : 4 * p + 4, 384:]]
            dst[8 + p] = jnp.concatenate(piece, axis=0).astype(BF)

    @pl.when(moves)
    def _():
        own_down(dsend)

    @pl.when(jnp.logical_not(moves))
    def _():
        own_down(sud.at[z, x, c, 1])

    change = remote(dsend, sud.at[pz, x, c, 1], ps.at[0], pr.at[0], swap)

    @pl.when(moves)
    def _():
        change.start()

    order = [0, 7, 1, 6, 2, 5, 3, 4]
    last = ((4, 3), (3, 4))

    def came(way, k):
        return (z + (NZ - k if way == 0 else k)) % NZ

    def place(way, k):
        return 7 if k == 4 else 2 * k - 1 + way

    def ud_z(q, way, k):
        block = sud.at[came(way, k), x, c, q]
        return remote(block, block, us.at[way], ur.at[(q * 2 + way) * 4 + k], (z_next, z_prev)[way])

    def ud_x(q, o, way):
        block = sud.at[(z + order[o]) % NZ, x, c, q]
        return remote(block, block, uxs.at[0], uxr.at[(q * 8 + o) * 2 + way], (x_next, x_prev)[way])

    def ud_f(q, o):
        block = sud.at[(z + order[o]) % NZ, (xm, xp)[q], c, q]
        return remote(block, block, ufs.at[0], ufr.at[q * 8 + o], (x_next, x_prev)[q])

    def g_z(way, k, e):
        block = sg.at[came(way, k), (x, xp, xm, x2)[e], c]
        return remote(block, block, gzs.at[way], gzr.at[(way * 4 + k) * 2 + e // 2], (z_next, z_prev)[way])

    def g_pair(way, k, h):
        block = sg.at[came(way, k), pl.ds(0, 2), c]
        return remote(block, block, gzs.at[way], gzr.at[(way * 4 + k) * 2 + h], (z_next, z_prev)[way])

    def g_twin(o):
        block = sg.at[(z + order[o]) % NZ, :, c]
        return remote(block, block, ds_.at[2], dr.at[2], twin)

    def ud_twin(q, o):
        block = sud.at[(z + order[o]) % NZ, :, c, q]
        return remote(block, block, ds_.at[q], dr.at[q], twin)

    def twins(n):
        block = sg.at[:, :, c] if n == 2 else sud.at[:, :, c, n]
        return remote(block, block, ds_.at[n], dr.at[n], twin)

    def ud_arrived(q, o):
        for way in range(2):
            ud_x(q, o, way).start()

    def ud_round(q, k):
        for way in range(2):
            if k <= last[q][way]:
                ud_z(q, way, k - 1).wait_recv()
                if k < last[q][way]:
                    ud_z(q, way, k).start()
                ud_arrived(q, place(way, k))

    def g_round(k, *hs):
        for h in hs:
            for way in range(2):
                if k < 4 or h == way:
                    g_pair(way, k - 1, h).wait_recv()
                    if k < 3 or k == 3 and h == way:
                        for e in (2 * h, 2 * h + 1):
                            g_z(way, k, e).start()
                    if h == 1:
                        g_twin(place(way, k)).start()

    def x_pass(q, *os):
        for o in os:
            for way in (q, 1 - q):
                ud_x(q, o, way).wait_recv()
                if way == q:
                    ud_f(q, o).start()

    def x_end(q, *os):
        for o in os:
            ud_f(q, o).wait_recv()
            ud_twin(q, o).start()

    def g_x(way):
        block = sg.at[z, x, c]
        return remote(block, block, gxs.at[0], gxr.at[way], (x_next, x_prev)[way])

    def g_far(way):
        block = sg.at[z, (xm, xp)[way], c, (pl.ds(0, 6), pl.ds(6, 5))[way]]
        return remote(block, block, gxs.at[0], gxr.at[2], (x_next, x_prev)[way])

    def shards_of(n, send, recv):
        block = sg.at[z, pl.ds(0, n), c]
        return remote(block, block, send, recv, x_next)

    for way in range(2):
        ud_z(0, way, 0).start()
    for way in range(2):
        g_x(way).start()
    ud_arrived(0, 0)
    for way in range(2):
        g_z(way, 0, 0).start()

    with jax.named_scope("change"):

        @pl.when(moves)
        def _():
            change.wait_recv()

    for way in range(2):
        ud_z(1, way, 0).start()
    ud_arrived(1, 0)
    with jax.named_scope("round_1"):
        for way in range(2):
            g_x(way).wait_recv()
            g_far(way).start()
        ud_round(0, 1)
        for e in (1, 2):
            for way in range(2):
                g_z(way, 0, e).start()
        x_pass(0, 0)
        shards_of(1, gxs.at[0], gxr.at[2]).wait_recv()
        for way in range(2):
            g_z(way, 0, 3).start()
        g_twin(0).start()
    with jax.named_scope("round_2"):
        ud_round(0, 2)
        g_round(1, 0)
        ud_round(1, 1)
        x_pass(0, 1, 2)
        g_round(1, 1)
        x_pass(1, 0)
        token_pass(0)
    with jax.named_scope("round_3"):
        ud_round(0, 3)
        g_round(2, 0)
        ud_round(1, 2)
        x_pass(0, 3, 4)
        g_round(2, 1)
        x_pass(1, 1, 2)
        x_end(0, 0)
    with jax.named_scope("round_4"):
        ud_round(0, 4)
        g_round(3, 0)
        ud_round(1, 3)
        x_pass(0, 5, 6)
        g_round(3, 1)
        token_pass(1)
        x_pass(1, 3, 4)
        x_end(0, 1, 2)
        x_end(1, 0)
    with jax.named_scope("round_5"):
        ud_round(1, 4)
        x_pass(0, 7)
        g_round(4, 0, 1)
        token_pass(2)
        x_end(0, 3, 4)
        x_pass(1, 5, 6)
        x_end(1, 1, 2)
    with jax.named_scope("round_6"):
        x_end(0, 5, 6)
        x_pass(1, 7)
        token_pass(3)
        x_end(1, 3, 4)
    with jax.named_scope("round_7"):
        x_end(0, 7)
        x_end(1, 5, 6)
    own_tokens.wait()

    def normalise(j):
        for k in range(PIECES):

            @pl.when(j == k * (PIECE // CHUNK))
            def _(k=k):
                for way in range(2):
                    token_forward(way, k).wait_recv()

        def rows_of(t, carry):
            rows = pl.ds(pl.multiple_of(j * CHUNK + t * 32, 32), 32)
            total = jnp.zeros((32, 1), F32)
            for b in range(NY):
                v = xs[b, rows, :].astype(F32)
                total = total + jnp.sum(v * v, axis=1, keepdims=True)
            r = lax.rsqrt(total / D + EPS)
            for b in range(NY):
                v = xs[b, rows, :].astype(F32)
                xn[pl.ds(pl.multiple_of(t * 32, 32), 32), pl.ds(b * COLS, COLS)] = (v * r).astype(BF)
            return carry

        lax.fori_loop(0, CHUNK // 32, rows_of, 0)

    def columns(q, n, pairs):
        zs, rows = pl.ds(2 * pairs.start, 2 * pairs.size), pairs.size * D // 4
        halves = []
        for t in (2 * n, 2 * n + 1):
            pair = pl.ds(2 * t, 2)
            if t == 5:
                half = ends[q, zs]
            elif q == 0:
                half = sud[zs, :, :, 0, pair]
            else:
                half = sg[zs, :, :, pair]
            halves.append(half.reshape(rows, 128))
        return jnp.concatenate(halves, axis=1)

    def first():
        for n in range(3):
            gate = jnp.dot(xn[...], columns(1, n, pl.ds(0, 4)), preferred_element_type=F32)
            up = jnp.dot(xn[...], columns(0, n, pl.ds(0, 4)), preferred_element_type=F32)
            hid[:, pl.ds(256 * n, 256)] = (gate / (1.0 + jnp.exp(-gate)) * up).astype(BF)

    def spread(n, carry):
        left = lax.broadcasted_iota(jnp.int32, (NX, NC, 16, 128), 3) < 64
        for q, tile in ((0, sud[n, :, :, 0, 10]), (1, sg[n, :, :, 10])):
            tile = tile.astype(F32)
            flat = tile.reshape(NX * NC * 16, 128)
            turned = pltpu.roll(flat, 64, 1).reshape(NX, NC, 16, 128)
            ends[q, n, :, :, 0] = jnp.where(left, tile, 0.0).astype(BF)
            ends[q, n, :, :, 1] = jnp.where(left, turned, 0.0).astype(BF)
        return carry

    def message(kind, way, j):
        rows = {"far": 1 - way, "near": way, "comb": 1 - way}[kind]
        to_block = y2 if kind == "far" else (yp, ym)[way]
        src = sums.at[j, way] if kind == "comb" else part.at[j, to_block, pl.ds(rows * HALF, HALF)]
        dst = {"far": far.at[j, way], "near": got.at[j, way], "comb": got.at[j, 2 + way]}[kind]
        return remote(src, dst, rs.at[0], rr.at[j + (0 if kind == "far" else CHUNKS)], (y_next, y_prev)[way])

    def all_far(j):
        return remote(sums.at[j], far.at[j], rs.at[0], rr.at[j], y_next)

    def all_got(j):
        return remote(got.at[j], got.at[j], rs.at[0], rr.at[CHUNKS + j], y_next)

    def second(j):
        def block(n, carry):
            b = (y + 2 + n) % NY
            cols = pl.ds(pl.multiple_of(b * COLS, COLS), COLS)
            part[j, b] = jnp.dot(hid[...], df[:, cols], preferred_element_type=F32).astype(BF)

            @pl.when(n == 0)
            def _():
                for way in range(2):
                    message("far", way, j).start()

            return carry

        lax.fori_loop(0, NY, block, 0)
        for way in range(2):
            message("near", way, j).start()

    def combine(j):
        all_far(j).wait_recv()
        for way in range(2):
            mine = part[j, (yp, ym)[way], pl.ds((1 - way) * HALF, HALF), :].astype(F32)
            sums[j, way] = (mine + far[j, way].astype(F32)).astype(BF)
        for way in range(2):
            message("comb", way, j).start()

    with jax.named_scope("normalise_0"):
        normalise(0)
    with jax.named_scope("wait_up"):
        x_end(1, 7)
        twins(2).wait_recv()
        twins(0).wait_recv()
    with jax.named_scope("first_0"):
        lax.fori_loop(0, NZ, spread, 0)
        first()
    with jax.named_scope("wait_down"):
        twins(1).wait_recv()

    def assemble(n, carry):
        a, group = n // 4, n % 4
        for s in range(4):
            shard = sud.at[2 * a + group // 2, (group % 2) * 2 + s // 2, s % 2, 1]
            at_row = DROWS * s
            for t in range(4):
                for r in range(2):
                    tmp[pl.ds(at_row + 16 * r, 16), pl.ds(128 * t, 128)] = shard[2 * t + r].astype(F32)
            for p in range(3):
                piece = shard[8 + p].astype(F32)
                tmp[pl.ds(at_row + ROWS, 12), pl.ds(128 * p, 128)] = piece[:12]
                tmp[pl.ds(at_row + ROWS + 4 * p, 4), pl.ds(384, 128)] = piece[12:]
        rows = pl.ds(pl.multiple_of(group * 176, 16), 176)
        df[rows, pl.ds(pl.multiple_of(a * COLS, COLS), COLS)] = tmp[...].astype(BF)
        return carry

    with jax.named_scope("assemble"):
        df[pl.ds(HID, WIDE - HID), :] = jnp.zeros((WIDE - HID, D), BF)
        lax.fori_loop(0, 16, assemble, 0)

    one = lax.broadcasted_iota(jnp.int32, (256, 256), 0) == lax.broadcasted_iota(jnp.int32, (256, 256), 1)
    unit = one.astype(F32).astype(BF)

    def turn_over(quarter):
        to = pl.ds(pl.multiple_of(quarter * 512, 512), 512)
        for n in range(3):
            for q, dst in ((0, ut), (1, gt)):
                dst[pl.ds(256 * n, 256), to] = lax.dot_general(
                    unit, columns(q, n, pl.ds(quarter, 1)), (((1,), (1,)), ((), ())), preferred_element_type=F32
                ).astype(BF)

    def step(j, carry):
        @pl.when(j < CHUNKS)
        def _():
            with jax.named_scope("second"):
                second(j)

        @pl.when(j > 0)
        def _():
            with jax.named_scope("combine"):
                combine(j - 1)

        @pl.when(j < CHUNKS - 1)
        def _():
            with jax.named_scope("first"):
                normalise(j + 1)
                first()

        @pl.when(jnp.logical_and(j >= 3, j < 7))
        def _():
            with jax.named_scope("turn_over"):
                turn_over(j - 3)

        return carry

    lax.fori_loop(0, CHUNKS + 1, step, 0)

    def finish(j, carry):
        all_got(j).wait_recv()
        for half in range(2):
            mine = part[j, y, pl.ds(half * HALF, HALF), :].astype(F32)
            total = mine + got[j, half].astype(F32) + got[j, 3 - half].astype(F32)
            out[pl.ds(pl.multiple_of(j * CHUNK + half * HALF, HALF), HALF), :] = total.astype(BF)
        return carry

    with jax.named_scope("finish"):
        lax.fori_loop(0, CHUNKS, finish, 0)

    with jax.named_scope("drain"):

        @pl.when(moves)
        def _():
            change.wait_send()

        shards_of(3, gxs.at[0], gxr.at[0]).wait_send()
        for way in range(2):
            block = sg.at[pl.ds(0, 7), x, c]
            remote(block, block, us.at[way], ur.at[0], z_next).wait_send()
            block = sg.at[pl.ds(0, 7), x]
            remote(block, block, gzs.at[way], gzr.at[0], z_next).wait_send()
            remote(tok, xs.at[y], ts.at[way], tr.at[0], y_next).wait_send()
            half = xs.at[0, pl.ds(0, PIECE * PIECES // 2)]
            remote(half, half, tfs.at[way], tfr.at[0], y_next).wait_send()
        block = sg.at[:, :, c]
        remote(block, block, uxs.at[0], uxr.at[0], x_next).wait_send()
        block = sg.at[pl.ds(0, 4), :, c]
        remote(block, block, ufs.at[0], ufr.at[0], x_next).wait_send()
        for n in range(3):
            twins(n).wait_send()
        block = xs.at[pl.ds(0, 3)]
        remote(block, block, rs.at[0], rr.at[0], y_next).wait_send()


def hand_out(gt, ut, df, out, go, uo, do, mo, sem):
    rows = pl.ds(0, HID)
    moved = ((gt.at[rows], go), (ut.at[rows], uo), (df.at[rows], do), (out, mo))
    copies = [pltpu.make_async_copy(src, dst, sem.at[n]) for n, (src, dst) in enumerate(moved)]
    for copy in copies:
        copy.start()
    for copy in copies:
        copy.wait()


def shards(tokens, norm_gain, gate_weight, up_weight, down_weight):
    vmem = functools.partial(pltpu.VMEM, dtype=BF)
    sem = pltpu.SemaphoreType.DMA
    hbm = pl.BlockSpec(memory_space=pltpu.HBM)
    held = pl.pallas_call(
        kernel,
        name="layer",
        out_shape=(jax.ShapeDtypeStruct((WIDE, D), BF),) * 3 + (jax.ShapeDtypeStruct((CHUNK * CHUNKS, COLS), BF),),
        in_specs=[hbm] + [pl.BlockSpec(memory_space=pltpu.VMEM)] * 3,
        out_specs=(pl.BlockSpec(memory_space=pltpu.VMEM),) * 4,
        scratch_shapes=[
            vmem((NY, CHUNK * CHUNKS, COLS)),
            vmem((NZ, NX, NC, TILES, 16, 128)),
            vmem((NZ, NX, NC, 2, TILES, 16, 128)),
            vmem((2, NZ, NX, NC, 2, 16, 128)),
            vmem((TILES, 16, 128)),
            pltpu.VMEM((4 * DROWS, COLS), F32),
            vmem((CHUNK, D)),
            vmem((CHUNK, WIDE)),
            vmem((CHUNKS, NY, CHUNK, COLS)),
            vmem((CHUNKS, 2, HALF, COLS)),
            vmem((CHUNKS, 4, HALF, COLS)),
            vmem((CHUNKS, 2, HALF, COLS)),
            sem((1,)), sem((1,)),
            sem((1,)), sem((3,)),
            sem((2,)), sem((16,)),
            sem((2,)), sem((16,)),
            sem((1,)), sem((32,)),
            sem((1,)), sem((16,)),
            sem((3,)), sem((3,)),
            sem((2,)), sem((2 * PIECES,)),
            sem((2,)), sem((2 * PIECES,)),
            sem((1,)), sem((2 * CHUNKS,)),
            sem((1,)),
        ],
        compiler_params=pltpu.CompilerParams(collective_id=0, has_side_effects=True, vmem_limit_bytes=LIMIT),
    )(
        tokens,
        (norm_gain[:, None] * gate_weight).astype(BF),
        (norm_gain[:, None] * up_weight).astype(BF),
        down_weight.astype(BF),
    )
    gate, up, down, mixed = pl.pallas_call(
        hand_out,
        name="hand_out",
        out_shape=(jax.ShapeDtypeStruct((HID, D), BF),) * 3 + (jax.ShapeDtypeStruct((CHUNK * CHUNKS, COLS), BF),),
        in_specs=[pl.BlockSpec(memory_space=pl.ANY)] * 4,
        out_specs=(hbm,) * 4,
        scratch_shapes=[sem((4,))],
        compiler_params=pltpu.CompilerParams(vmem_limit_bytes=2**20),
    )(*held)
    return (gate.T, up.T, down, mixed)


def solution(mesh):
    return jax.shard_map(
        shards,
        mesh=mesh,
        in_specs=(P("fs", "tp"), P("fs"), P("fs", "tp"), P("fs", "tp"), P("fs", "tp")),
        out_specs=(P(None, "tp"), P(None, "tp"), P("tp", None), P("fs", "tp")),
        check_vma=False,
    )
```

```python
import functools

import jax
import jax.numpy as jnp
from jax import lax
from jax.experimental import pallas as pl
from jax.experimental.pallas import tpu as pltpu
from jax.sharding import PartitionSpec as P

MESH = pl.DeviceIdType.MESH
BF = jnp.bfloat16
F32 = jnp.float32
NZ, NX, NC, NY = 8, 4, 2, 4
ROWS = 32
HID = 704
WIDE = 768
TILES = 11
DROWS, COLS = 44, 512
D = 2048
CHUNK, CHUNKS = 128, 8
PIECE, PIECES = 256, 4
HALF = CHUNK // 2
EPS = 1e-06
LIMIT = 38 * 2**20


def kernel(
    tok, gw, uw, dw,
    gt, ut, df, out,
    xs, sg, sud, ends, dsend, tmp, xn, hid, part, far, got, sums,
    ps, pr, gxs, gxr, gzs, gzr, us, ur, uxs, uxr, ufs, ufr, ds_, dr, ts, tr, tfs, tfr, rs, rr, loc,
):
    f, y = lax.axis_index("fs"), lax.axis_index("tp")
    z, x, c = f // 8, (f // 2) % 4, f % 2
    za, zb = z // 2, z % 2

    def at(zz, xx, cc, yy):
        return ((zz * NX + xx) * NC + cc, yy)

    zp, zm = (z + 1) % NZ, (z + 7) % NZ
    xp, xm, x2 = (x + 1) % NX, (x + 3) % NX, (x + 2) % NX
    yp, ym, y2 = (y + 1) % NY, (y + 3) % NY, (y + 2) % NY
    z_next, z_prev = at(zp, x, c, y), at(zm, x, c, y)
    x_next, x_prev, x_far = at(z, xp, c, y), at(z, xm, c, y), at(z, x2, c, y)
    y_next, y_prev = at(z, x, c, yp), at(z, x, c, ym)
    twin = at(z, x, 1 - c, y)
    pz = 2 * y + zb
    swap = at(pz, x, c, za)
    moves = za != y

    def remote(src, dst, send, recv, device):
        return pltpu.make_async_remote_copy(
            src_ref=src, dst_ref=dst, send_sem=send, recv_sem=recv, device_id=device, device_id_type=MESH
        )

    own_tokens = pltpu.make_async_copy(tok, xs.at[y], loc.at[0])

    barrier = pltpu.get_barrier_semaphore()
    for partner in (z_next, z_prev, x_next, x_prev, x_far, y_next, y_prev, twin):
        pl.semaphore_signal(barrier, inc=1, device_id=partner, device_id_type=MESH)

    @pl.when(moves)
    def _():
        pl.semaphore_signal(barrier, inc=1, device_id=swap, device_id_type=MESH)

    for ref, dst in ((uw, sud.at[z, x, c, 0]), (gw, sg.at[z, x, c])):
        for t in range(5):
            for r in range(2):
                dst[2 * t + r] = ref[pl.ds(16 * r, 16), pl.ds(128 * t, 128)]
        dst[10] = jnp.concatenate([ref[pl.ds(16 * r, 16), pl.ds(640, 64)] for r in range(2)], axis=1)

    def own_down(dst):
        for t in range(4):
            for r in range(2):
                dst[2 * t + r] = dw[pl.ds(16 * r, 16), pl.ds(128 * t, 128)]
        low = dw[pl.ds(ROWS, DROWS - ROWS), :].astype(F32)
        for p in range(3):
            piece = [low[:, 128 * p : 128 * p + 128], low[4 * p : 4 * p + 4, 384:]]
            dst[8 + p] = jnp.concatenate(piece, axis=0).astype(BF)

    @pl.when(moves)
    def _():
        own_down(dsend)

    @pl.when(jnp.logical_not(moves))
    def _():
        own_down(sud.at[z, x, c, 1])

    with jax.named_scope("meet"):
        pl.semaphore_wait(barrier, 8 + moves.astype(jnp.int32))

    change = remote(dsend, sud.at[pz, x, c, 1], ps.at[0], pr.at[0], swap)

    @pl.when(moves)
    def _():
        change.start()

    def token_copy(way, j):
        rows = pl.ds(j * PIECE, PIECE)
        return remote(tok.at[rows], xs.at[y, rows], ts.at[way], tr.at[way * PIECES + j], (y_next, y_prev)[way])

    def token_forward(way, j):
        rows = pl.ds(j * PIECE + way * (PIECE // 2), PIECE // 2)
        block = xs.at[(ym, yp)[way], rows]
        return remote(block, block, tfs.at[way], tfr.at[way * PIECES + j], (y_next, y_prev)[way])

    def token_pass(j):
        for way in range(2):
            token_copy(way, j).wait_recv()
            token_forward(way, j).start()

    for j in range(PIECES):
        for way in range(2):
            token_copy(way, j).start()
    own_tokens.start()

    order = [0, 7, 1, 6, 2, 5, 3, 4]
    last = ((4, 3), (3, 4))

    def came(way, k):
        return (z + (NZ - k if way == 0 else k)) % NZ

    def place(way, k):
        return 7 if k == 4 else 2 * k - 1 + way

    def ud_z(q, way, k):
        block = sud.at[came(way, k), x, c, q]
        return remote(block, block, us.at[way], ur.at[(q * 2 + way) * 4 + k], (z_next, z_prev)[way])

    def ud_x(q, o, way):
        block = sud.at[(z + order[o]) % NZ, x, c, q]
        return remote(block, block, uxs.at[0], uxr.at[(q * 8 + o) * 2 + way], (x_next, x_prev)[way])

    def ud_f(q, o):
        block = sud.at[(z + order[o]) % NZ, (xm, xp)[q], c, q]
        return remote(block, block, ufs.at[0], ufr.at[q * 8 + o], (x_next, x_prev)[q])

    def g_z(way, k, e):
        block = sg.at[came(way, k), (x, xp, xm, x2)[e], c]
        return remote(block, block, gzs.at[way], gzr.at[(way * 4 + k) * 2 + e // 2], (z_next, z_prev)[way])

    def g_pair(way, k, h):
        block = sg.at[came(way, k), pl.ds(0, 2), c]
        return remote(block, block, gzs.at[way], gzr.at[(way * 4 + k) * 2 + h], (z_next, z_prev)[way])

    def g_twin(o, e):
        block = sg.at[(z + order[o]) % NZ, (x, xp, xm, x2)[e], c]
        return remote(block, block, ds_.at[2], dr.at[2], twin)

    def ud_twin(q, o, e):
        block = sud.at[(z + order[o]) % NZ, (x, xp, xm, x2)[e], c, q]
        return remote(block, block, ds_.at[q], dr.at[q], twin)

    def twins(n):
        block = sg.at[:, :, c] if n == 2 else sud.at[:, :, c, n]
        return remote(block, block, ds_.at[n], dr.at[n], twin)

    def ud_arrived(q, o):
        for way in range(2):
            ud_x(q, o, way).start()

    def ud_round(q, k):
        for way in range(2):
            if k <= last[q][way]:
                ud_z(q, way, k - 1).wait_recv()
                if k < last[q][way]:
                    ud_z(q, way, k).start()
                ud_arrived(q, place(way, k))

    def g_round(k, *hs):
        for h in hs:
            for way in range(2):
                if k < 4 or h == way:
                    g_pair(way, k - 1, h).wait_recv()
                    if k < 3 or k == 3 and h == way:
                        for e in (2 * h, 2 * h + 1):
                            g_z(way, k, e).start()
                    for e in (2 * h, 2 * h + 1):
                        g_twin(place(way, k), e).start()

    def x_pass(q, *os):
        for o in os:
            for way in (q, 1 - q):
                ud_x(q, o, way).wait_recv()
                if way == q:
                    ud_f(q, o).start()
            for e in range(3):
                ud_twin(q, o, e).start()

    def x_end(q, *os):
        for o in os:
            ud_f(q, o).wait_recv()
            ud_twin(q, o, 3).start()

    def g_x(way):
        block = sg.at[z, x, c]
        return remote(block, block, gxs.at[0], gxr.at[way], (x_next, x_prev)[way])

    def g_far(way):
        block = sg.at[z, (xm, xp)[way], c, (pl.ds(0, 6), pl.ds(6, 5))[way]]
        return remote(block, block, gxs.at[0], gxr.at[2], (x_next, x_prev)[way])

    def shards_of(n, send, recv):
        block = sg.at[z, pl.ds(0, n), c]
        return remote(block, block, send, recv, x_next)

    for way in range(2):
        ud_z(0, way, 0).start()
    for way in range(2):
        g_x(way).start()
    ud_arrived(0, 0)
    for way in range(2):
        g_z(way, 0, 0).start()

    with jax.named_scope("change"):

        @pl.when(moves)
        def _():
            change.wait_recv()

    for way in range(2):
        ud_z(1, way, 0).start()
    ud_arrived(1, 0)
    with jax.named_scope("round_1"):
        for way in range(2):
            g_x(way).wait_recv()
            g_far(way).start()
        ud_round(0, 1)
        for e in (1, 2):
            for way in range(2):
                g_z(way, 0, e).start()
        x_pass(0, 0)
        shards_of(1, gxs.at[0], gxr.at[2]).wait_recv()
        for way in range(2):
            g_z(way, 0, 3).start()
        for e in range(4):
            g_twin(0, e).start()
    with jax.named_scope("round_2"):
        ud_round(0, 2)
        g_round(1, 0)
        ud_round(1, 1)
        x_pass(0, 1, 2)
        g_round(1, 1)
        x_pass(1, 0)
        token_pass(0)
    with jax.named_scope("round_3"):
        ud_round(0, 3)
        g_round(2, 0)
        ud_round(1, 2)
        x_pass(0, 3, 4)
        g_round(2, 1)
        x_pass(1, 1, 2)
        x_end(0, 0, 1, 2)
        x_end(1, 0)
    with jax.named_scope("round_4"):
        ud_round(0, 4)
        g_round(3, 0)
        ud_round(1, 3)
        x_pass(0, 5, 6)
        g_round(3, 1)
        x_pass(0, 7)
        token_pass(1)
        x_pass(1, 3, 4)
        x_end(0, 3, 4)
    with jax.named_scope("round_5"):
        ud_round(1, 4)
        g_round(4, 0, 1)
        token_pass(2)
        x_pass(1, 5, 6)
        x_end(0, 5, 6)
        x_end(1, 1, 2)
    with jax.named_scope("round_6"):
        x_pass(1, 7)
        token_pass(3)
        x_end(0, 7)
        x_end(1, 3, 4)
    own_tokens.wait()

    def normalise(j):
        for k in range(PIECES):

            @pl.when(j == k * (PIECE // CHUNK))
            def _(k=k):
                for way in range(2):
                    token_forward(way, k).wait_recv()

        def rows_of(t, carry):
            rows = pl.ds(pl.multiple_of(j * CHUNK + t * 32, 32), 32)
            total = jnp.zeros((32, 1), F32)
            for b in range(NY):
                v = xs[b, rows, :].astype(F32)
                total = total + jnp.sum(v * v, axis=1, keepdims=True)
            r = lax.rsqrt(total / D + EPS)
            for b in range(NY):
                v = xs[b, rows, :].astype(F32)
                xn[pl.ds(pl.multiple_of(t * 32, 32), 32), pl.ds(b * COLS, COLS)] = (v * r).astype(BF)
            return carry

        lax.fori_loop(0, CHUNK // 32, rows_of, 0)

    def columns(q, n, pairs):
        zs, rows = pl.ds(2 * pairs.start, 2 * pairs.size), pairs.size * D // 4
        halves = []
        for t in (2 * n, 2 * n + 1):
            pair = pl.ds(2 * t, 2)
            if t == 5:
                half = ends[q, zs]
            elif q == 0:
                half = sud[zs, :, :, 0, pair]
            else:
                half = sg[zs, :, :, pair]
            halves.append(half.reshape(rows, 128))
        return jnp.concatenate(halves, axis=1)

    def first(ns):
        for n in ns:
            gate = jnp.dot(xn[...], columns(1, n, pl.ds(0, 4)), preferred_element_type=F32)
            up = jnp.dot(xn[...], columns(0, n, pl.ds(0, 4)), preferred_element_type=F32)
            hid[:, pl.ds(256 * n, 256)] = (gate / (1.0 + jnp.exp(-gate)) * up).astype(BF)

    def spread(n, carry):
        left = lax.broadcasted_iota(jnp.int32, (NX, NC, 16, 128), 3) < 64
        for q, tile in ((0, sud[n, :, :, 0, 10]), (1, sg[n, :, :, 10])):
            tile = tile.astype(F32)
            flat = tile.reshape(NX * NC * 16, 128)
            turned = pltpu.roll(flat, 64, 1).reshape(NX, NC, 16, 128)
            ends[q, n, :, :, 0] = jnp.where(left, tile, 0.0).astype(BF)
            ends[q, n, :, :, 1] = jnp.where(left, turned, 0.0).astype(BF)
        return carry

    def message(kind, way, j):
        rows = {"far": 1 - way, "near": way, "comb": 1 - way}[kind]
        to_block = y2 if kind == "far" else (yp, ym)[way]
        src = sums.at[j, way] if kind == "comb" else part.at[j, to_block, pl.ds(rows * HALF, HALF)]
        dst = {"far": far.at[j, way], "near": got.at[j, way], "comb": got.at[j, 2 + way]}[kind]
        return remote(src, dst, rs.at[0], rr.at[j + (0 if kind == "far" else CHUNKS)], (y_next, y_prev)[way])

    def all_far(j):
        return remote(sums.at[j], far.at[j], rs.at[0], rr.at[j], y_next)

    def all_got(j):
        return remote(got.at[j], got.at[j], rs.at[0], rr.at[CHUNKS + j], y_next)

    def second(j):
        def block(n, carry):
            b = (y + 2 + n) % NY
            cols = pl.ds(pl.multiple_of(b * COLS, COLS), COLS)
            part[j, b] = jnp.dot(hid[...], df[:, cols], preferred_element_type=F32).astype(BF)

            @pl.when(n == 0)
            def _():
                for way in range(2):
                    message("far", way, j).start()

            return carry

        lax.fori_loop(0, NY, block, 0)
        for way in range(2):
            message("near", way, j).start()

    def combine(j):
        all_far(j).wait_recv()
        for way in range(2):
            mine = part[j, (yp, ym)[way], pl.ds((1 - way) * HALF, HALF), :].astype(F32)
            sums[j, way] = (mine + far[j, way].astype(F32)).astype(BF)
        for way in range(2):
            message("comb", way, j).start()

    @pl.when(c == 1)
    def _():
        x_end(1, 5, 6, 7)

    with jax.named_scope("normalise_0"):
        normalise(0)
    with jax.named_scope("wait_up"):
        twins(2).wait_recv()
        twins(0).wait_recv()
    with jax.named_scope("first_0"):
        lax.fori_loop(0, NZ, spread, 0)
        first(range(3))

    with jax.named_scope("last_down"):

        @pl.when(c == 0)
        def _():
            x_end(1, 5, 6, 7)

    with jax.named_scope("wait_down"):
        twins(1).wait_recv()

    def assemble(n, carry):
        a, group = n // 4, n % 4
        for s in range(4):
            shard = sud.at[2 * a + group // 2, (group % 2) * 2 + s // 2, s % 2, 1]
            at_row = DROWS * s
            for t in range(4):
                for r in range(2):
                    tmp[pl.ds(at_row + 16 * r, 16), pl.ds(128 * t, 128)] = shard[2 * t + r].astype(F32)
            for p in range(3):
                piece = shard[8 + p].astype(F32)
                tmp[pl.ds(at_row + ROWS, 12), pl.ds(128 * p, 128)] = piece[:12]
                tmp[pl.ds(at_row + ROWS + 4 * p, 4), pl.ds(384, 128)] = piece[12:]
        rows = pl.ds(pl.multiple_of(group * 176, 16), 176)
        df[rows, pl.ds(pl.multiple_of(a * COLS, COLS), COLS)] = tmp[...].astype(BF)
        return carry

    with jax.named_scope("assemble"):
        df[pl.ds(HID, WIDE - HID), :] = jnp.zeros((WIDE - HID, D), BF)
        lax.fori_loop(0, 16, assemble, 0)

    one = lax.broadcasted_iota(jnp.int32, (256, 256), 0) == lax.broadcasted_iota(jnp.int32, (256, 256), 1)
    unit = one.astype(F32).astype(BF)

    def turn_over(quarter):
        to = pl.ds(pl.multiple_of(quarter * 512, 512), 512)
        for n in range(3):
            for q, dst in ((0, ut), (1, gt)):
                dst[pl.ds(256 * n, 256), to] = lax.dot_general(
                    unit, columns(q, n, pl.ds(quarter, 1)), (((1,), (1,)), ((), ())), preferred_element_type=F32
                ).astype(BF)

    def step(j, carry):
        @pl.when(j < CHUNKS)
        def _():
            with jax.named_scope("second"):
                second(j)

        @pl.when(j > 0)
        def _():
            with jax.named_scope("combine"):
                combine(j - 1)

        @pl.when(j < CHUNKS - 1)
        def _():
            with jax.named_scope("first"):
                normalise(j + 1)
                first(range(3))

        @pl.when(jnp.logical_and(j >= 3, j < 7))
        def _():
            with jax.named_scope("turn_over"):
                turn_over(j - 3)

        return carry

    lax.fori_loop(0, CHUNKS + 1, step, 0)

    def finish(j, carry):
        all_got(j).wait_recv()
        for half in range(2):
            mine = part[j, y, pl.ds(half * HALF, HALF), :].astype(F32)
            total = mine + got[j, half].astype(F32) + got[j, 3 - half].astype(F32)
            out[pl.ds(pl.multiple_of(j * CHUNK + half * HALF, HALF), HALF), :] = total.astype(BF)
        return carry

    with jax.named_scope("finish"):
        lax.fori_loop(0, CHUNKS, finish, 0)

    with jax.named_scope("drain"):

        @pl.when(moves)
        def _():
            change.wait_send()

        shards_of(3, gxs.at[0], gxr.at[0]).wait_send()
        for way in range(2):
            block = sg.at[pl.ds(0, 7), x, c]
            remote(block, block, us.at[way], ur.at[0], z_next).wait_send()
            block = sg.at[pl.ds(0, 7), x]
            remote(block, block, gzs.at[way], gzr.at[0], z_next).wait_send()
            remote(tok, xs.at[y], ts.at[way], tr.at[0], y_next).wait_send()
            half = xs.at[0, pl.ds(0, PIECE * PIECES // 2)]
            remote(half, half, tfs.at[way], tfr.at[0], y_next).wait_send()
        block = sg.at[:, :, c]
        remote(block, block, uxs.at[0], uxr.at[0], x_next).wait_send()
        block = sg.at[pl.ds(0, 4), :, c]
        remote(block, block, ufs.at[0], ufr.at[0], x_next).wait_send()
        for n in range(3):
            twins(n).wait_send()
        block = xs.at[pl.ds(0, 3)]
        remote(block, block, rs.at[0], rr.at[0], y_next).wait_send()


def hand_out(gt, ut, df, out, go, uo, do, mo, sem):
    rows = pl.ds(0, HID)
    moved = ((gt.at[rows], go), (ut.at[rows], uo), (df.at[rows], do), (out, mo))
    copies = [pltpu.make_async_copy(src, dst, sem.at[n]) for n, (src, dst) in enumerate(moved)]
    for copy in copies:
        copy.start()
    for copy in copies:
        copy.wait()


def shards(tokens, norm_gain, gate_weight, up_weight, down_weight):
    vmem = functools.partial(pltpu.VMEM, dtype=BF)
    sem = pltpu.SemaphoreType.DMA
    hbm = pl.BlockSpec(memory_space=pltpu.HBM)
    held = pl.pallas_call(
        kernel,
        name="layer",
        out_shape=(jax.ShapeDtypeStruct((WIDE, D), BF),) * 3 + (jax.ShapeDtypeStruct((CHUNK * CHUNKS, COLS), BF),),
        in_specs=[hbm] + [pl.BlockSpec(memory_space=pltpu.VMEM)] * 3,
        out_specs=(pl.BlockSpec(memory_space=pltpu.VMEM),) * 4,
        scratch_shapes=[
            vmem((NY, CHUNK * CHUNKS, COLS)),
            vmem((NZ, NX, NC, TILES, 16, 128)),
            vmem((NZ, NX, NC, 2, TILES, 16, 128)),
            vmem((2, NZ, NX, NC, 2, 16, 128)),
            vmem((TILES, 16, 128)),
            pltpu.VMEM((4 * DROWS, COLS), F32),
            vmem((CHUNK, D)),
            vmem((CHUNK, WIDE)),
            vmem((CHUNKS, NY, CHUNK, COLS)),
            vmem((CHUNKS, 2, HALF, COLS)),
            vmem((CHUNKS, 4, HALF, COLS)),
            vmem((CHUNKS, 2, HALF, COLS)),
            sem((1,)), sem((1,)),
            sem((1,)), sem((3,)),
            sem((2,)), sem((16,)),
            sem((2,)), sem((16,)),
            sem((1,)), sem((32,)),
            sem((1,)), sem((16,)),
            sem((3,)), sem((3,)),
            sem((2,)), sem((2 * PIECES,)),
            sem((2,)), sem((2 * PIECES,)),
            sem((1,)), sem((2 * CHUNKS,)),
            sem((1,)),
        ],
        compiler_params=pltpu.CompilerParams(collective_id=0, has_side_effects=True, vmem_limit_bytes=LIMIT),
    )(
        tokens,
        (norm_gain[:, None] * gate_weight).astype(BF),
        (norm_gain[:, None] * up_weight).astype(BF),
        down_weight.astype(BF),
    )
    gate, up, down, mixed = pl.pallas_call(
        hand_out,
        name="hand_out",
        out_shape=(jax.ShapeDtypeStruct((HID, D), BF),) * 3 + (jax.ShapeDtypeStruct((CHUNK * CHUNKS, COLS), BF),),
        in_specs=[pl.BlockSpec(memory_space=pl.ANY)] * 4,
        out_specs=(hbm,) * 4,
        scratch_shapes=[sem((4,))],
        compiler_params=pltpu.CompilerParams(vmem_limit_bytes=2**20),
    )(*held)
    return (gate.T, up.T, down, mixed)


def solution(mesh):
    return jax.shard_map(
        shards,
        mesh=mesh,
        in_specs=(P("fs", "tp"), P("fs"), P("fs", "tp"), P("fs", "tp"), P("fs", "tp")),
        out_specs=(P(None, "tp"), P(None, "tp"), P("tp", None), P("fs", "tp")),
        check_vma=False,
    )
```

```python
import functools

import jax
import jax.numpy as jnp
from jax import lax
from jax.experimental import pallas as pl
from jax.experimental.pallas import tpu as pltpu
from jax.sharding import PartitionSpec as P

MESH = pl.DeviceIdType.MESH
BF = jnp.bfloat16
F32 = jnp.float32
NZ, NX, NC, NY = 8, 4, 2, 4
ROWS = 32
HID = 704
WIDE = 768
TILES = 11
DROWS, COLS = 44, 512
D = 2048
CHUNK, CHUNKS = 128, 8
PIECE, PIECES = 256, 4
HALF = CHUNK // 2
EPS = 1e-06
LIMIT = 38 * 2**20


def kernel(
    tok, gw, uw, dw,
    gt, ut, df, out,
    xs, sg, sud, ends, dsend, tmp, xn, hid, part, far, got, sums,
    ps, pr, gxs, gxr, gzs, gzr, us, ur, uxs, uxr, ufs, ufr, ds_, dr, ts, tr, tfs, tfr, rs, rr, zfs, zfr, loc,
):
    f, y = lax.axis_index("fs"), lax.axis_index("tp")
    z, x, c = f // 8, (f // 2) % 4, f % 2
    za, zb = z // 2, z % 2

    def at(zz, xx, cc, yy):
        return ((zz * NX + xx) * NC + cc, yy)

    zp, zm = (z + 1) % NZ, (z + 7) % NZ
    xp, xm, x2 = (x + 1) % NX, (x + 3) % NX, (x + 2) % NX
    yp, ym, y2 = (y + 1) % NY, (y + 3) % NY, (y + 2) % NY
    z_next, z_prev = at(zp, x, c, y), at(zm, x, c, y)
    x_next, x_prev, x_far = at(z, xp, c, y), at(z, xm, c, y), at(z, x2, c, y)
    y_next, y_prev = at(z, x, c, yp), at(z, x, c, ym)
    twin, z_far = at(z, x, 1 - c, y), at((z + 4) % NZ, x, c, y)
    pz = 2 * y + zb
    swap = at(pz, x, c, za)
    moves = za != y

    def remote(src, dst, send, recv, device):
        return pltpu.make_async_remote_copy(
            src_ref=src, dst_ref=dst, send_sem=send, recv_sem=recv, device_id=device, device_id_type=MESH
        )

    own_tokens = pltpu.make_async_copy(tok, xs.at[y], loc.at[0])

    barrier = pltpu.get_barrier_semaphore()
    for partner in (z_next, z_prev, z_far, x_next, x_prev, y_next, y_prev, twin):
        pl.semaphore_signal(barrier, inc=1, device_id=partner, device_id_type=MESH)

    @pl.when(moves)
    def _():
        pl.semaphore_signal(barrier, inc=1, device_id=swap, device_id_type=MESH)

    for ref, dst in ((uw, sud.at[z, x, c, 0]), (gw, sg.at[z, x, c])):
        for t in range(5):
            for r in range(2):
                dst[2 * t + r] = ref[pl.ds(16 * r, 16), pl.ds(128 * t, 128)]
        dst[10] = jnp.concatenate([ref[pl.ds(16 * r, 16), pl.ds(640, 64)] for r in range(2)], axis=1)

    def own_down(dst):
        for t in range(4):
            for r in range(2):
                dst[2 * t + r] = dw[pl.ds(16 * r, 16), pl.ds(128 * t, 128)]
        low = dw[pl.ds(ROWS, DROWS - ROWS), :].astype(F32)
        for p in range(3):
            piece = [low[:, 128 * p : 128 * p + 128], low[4 * p : 4 * p + 4, 384:]]
            dst[8 + p] = jnp.concatenate(piece, axis=0).astype(BF)

    @pl.when(moves)
    def _():
        own_down(dsend)

    @pl.when(jnp.logical_not(moves))
    def _():
        own_down(sud.at[z, x, c, 1])

    with jax.named_scope("meet"):
        pl.semaphore_wait(barrier, 8 + moves.astype(jnp.int32))

    change = remote(dsend, sud.at[pz, x, c, 1], ps.at[0], pr.at[0], swap)

    @pl.when(moves)
    def _():
        change.start()

    def token_copy(way, j):
        rows = pl.ds(j * PIECE, PIECE)
        return remote(tok.at[rows], xs.at[y, rows], ts.at[way], tr.at[way * PIECES + j], (y_next, y_prev)[way])

    def token_forward(way, j):
        rows = pl.ds(j * PIECE + way * (PIECE // 2), PIECE // 2)
        block = xs.at[(ym, yp)[way], rows]
        return remote(block, block, tfs.at[way], tfr.at[way * PIECES + j], (y_next, y_prev)[way])

    def token_pass(j):
        for way in range(2):
            token_copy(way, j).wait_recv()
            token_forward(way, j).start()

    for j in range(PIECES):
        for way in range(2):
            token_copy(way, j).start()
    own_tokens.start()

    order = [0, 7, 1, 6, 2, 5, 3, 4]
    last = ((3, 3), (3, 4))

    def came(way, k):
        return (z + (NZ - k if way == 0 else k)) % NZ

    def place(way, k):
        return 7 if k == 4 else 2 * k - 1 + way

    def ud_z(q, way, k):
        block = sud.at[came(way, k), x, c, q]
        return remote(block, block, us.at[way], ur.at[(q * 2 + way) * 4 + k], (z_next, z_prev)[way])

    def ud_x(q, o, way):
        block = sud.at[(z + order[o]) % NZ, x, c, q]
        return remote(block, block, uxs.at[0], uxr.at[(q * 8 + o) * 2 + way], (x_next, x_prev)[way])

    def ud_f(q, o):
        block = sud.at[(z + order[o]) % NZ, (xm, xp)[q], c, q]
        return remote(block, block, ufs.at[0], ufr.at[q * 8 + o], (x_next, x_prev)[q])

    def g_z(way, k, e):
        block = sg.at[came(way, k), (x, xp, xm, x2)[e], c]
        return remote(block, block, gzs.at[way], gzr.at[(way * 4 + k) * 2 + e // 2], (z_next, z_prev)[way])

    def g_pair(way, k, h):
        block = sg.at[came(way, k), pl.ds(0, 2), c]
        return remote(block, block, gzs.at[way], gzr.at[(way * 4 + k) * 2 + h], (z_next, z_prev)[way])

    def g_twin(o, e):
        block = sg.at[(z + order[o]) % NZ, (x, xp, xm, x2)[e], c]
        return remote(block, block, ds_.at[2], dr.at[2], twin)

    def ud_twin(q, o, e):
        block = sud.at[(z + order[o]) % NZ, (x, xp, xm, x2)[e], c, q]
        return remote(block, block, ds_.at[q], dr.at[q], twin)

    def twins(n):
        block = sg.at[:, :, c] if n == 2 else sud.at[:, :, c, n]
        return remote(block, block, ds_.at[n], dr.at[n], twin)

    def ud_arrived(q, o):
        for way in range(2):
            ud_x(q, o, way).start()

    def ud_round(q, k):
        for way in range(2):
            if k <= last[q][way]:
                ud_z(q, way, k - 1).wait_recv()
                if k < last[q][way]:
                    ud_z(q, way, k).start()
                ud_arrived(q, place(way, k))

    def g_round(k, *hs):
        for h in hs:
            for way in range(2):
                if k < 4 or h == way:
                    g_pair(way, k - 1, h).wait_recv()
                    if k < 3 or k == 3 and h == way:
                        for e in (2 * h, 2 * h + 1):
                            g_z(way, k, e).start()
                    for e in (2 * h, 2 * h + 1):
                        g_twin(place(way, k), e).start()

    def x_pass(q, *os):
        for o in os:
            for way in (q, 1 - q):
                ud_x(q, o, way).wait_recv()
                if way == q:
                    ud_f(q, o).start()
            for e in range(3):
                ud_twin(q, o, e).start()

    def x_end(q, *os):
        for o in os:
            ud_f(q, o).wait_recv()
            ud_twin(q, o, 3).start()

    def g_x(way):
        block = sg.at[z, x, c]
        return remote(block, block, gxs.at[0], gxr.at[way], (x_next, x_prev)[way])

    def g_far(way):
        block = sg.at[z, (xm, xp)[way], c, (pl.ds(0, 6), pl.ds(6, 5))[way]]
        return remote(block, block, gxs.at[0], gxr.at[2], (x_next, x_prev)[way])

    def shards_of(n, send, recv):
        block = sg.at[z, pl.ds(0, n), c]
        return remote(block, block, send, recv, x_next)

    own_up = sud.at[z, x, c, 0]
    far_up = remote(own_up, own_up, zfs.at[0], zfr.at[0], z_far)
    for way in range(2):
        ud_z(0, way, 0).start()
    for way in range(2):
        g_x(way).start()
    ud_arrived(0, 0)
    far_up.start()
    for way in range(2):
        g_z(way, 0, 0).start()

    with jax.named_scope("change"):

        @pl.when(moves)
        def _():
            change.wait_recv()

    for way in range(2):
        ud_z(1, way, 0).start()
    ud_arrived(1, 0)
    with jax.named_scope("round_1"):
        for way in range(2):
            g_x(way).wait_recv()
            g_far(way).start()
        ud_round(0, 1)
        for e in (1, 2):
            for way in range(2):
                g_z(way, 0, e).start()
        x_pass(0, 0)
        far_up.wait_recv()
        ud_arrived(0, 7)
        shards_of(1, gxs.at[0], gxr.at[2]).wait_recv()
        for way in range(2):
            g_z(way, 0, 3).start()
        for e in range(4):
            g_twin(0, e).start()
    with jax.named_scope("round_2"):
        ud_round(0, 2)
        g_round(1, 0)
        ud_round(1, 1)
        x_pass(0, 1, 2, 7)
        g_round(1, 1)
        x_pass(1, 0)
        token_pass(0)
    with jax.named_scope("round_3"):
        ud_round(0, 3)
        g_round(2, 0)
        ud_round(1, 2)
        x_pass(0, 3, 4)
        g_round(2, 1)
        x_pass(1, 1, 2)
        x_end(0, 0, 1, 2)
        x_end(1, 0)
    with jax.named_scope("round_4"):
        g_round(3, 0)
        ud_round(1, 3)
        x_pass(0, 5, 6)
        g_round(3, 1)
        token_pass(1)
        x_pass(1, 3, 4)
        x_end(0, 7, 3, 4)
    with jax.named_scope("round_5"):
        ud_round(1, 4)
        g_round(4, 0, 1)
        token_pass(2)
        x_pass(1, 5, 6)
        x_end(0, 5, 6)
        x_end(1, 1, 2)
    with jax.named_scope("round_6"):
        x_pass(1, 7)
        token_pass(3)
        x_end(1, 3, 4)
    own_tokens.wait()

    def normalise(j):
        for k in range(PIECES):

            @pl.when(j == k * (PIECE // CHUNK))
            def _(k=k):
                for way in range(2):
                    token_forward(way, k).wait_recv()

        def rows_of(t, carry):
            rows = pl.ds(pl.multiple_of(j * CHUNK + t * 32, 32), 32)
            total = jnp.zeros((32, 1), F32)
            for b in range(NY):
                v = xs[b, rows, :].astype(F32)
                total = total + jnp.sum(v * v, axis=1, keepdims=True)
            r = lax.rsqrt(total / D + EPS)
            for b in range(NY):
                v = xs[b, rows, :].astype(F32)
                xn[pl.ds(pl.multiple_of(t * 32, 32), 32), pl.ds(b * COLS, COLS)] = (v * r).astype(BF)
            return carry

        lax.fori_loop(0, CHUNK // 32, rows_of, 0)

    def columns(q, n, pairs):
        zs, rows = pl.ds(2 * pairs.start, 2 * pairs.size), pairs.size * D // 4
        halves = []
        for t in (2 * n, 2 * n + 1):
            pair = pl.ds(2 * t, 2)
            if t == 5:
                half = ends[q, zs]
            elif q == 0:
                half = sud[zs, :, :, 0, pair]
            else:
                half = sg[zs, :, :, pair]
            halves.append(half.reshape(rows, 128))
        return jnp.concatenate(halves, axis=1)

    def first(ns):
        for n in ns:
            gate = jnp.dot(xn[...], columns(1, n, pl.ds(0, 4)), preferred_element_type=F32)
            up = jnp.dot(xn[...], columns(0, n, pl.ds(0, 4)), preferred_element_type=F32)
            hid[:, pl.ds(256 * n, 256)] = (gate / (1.0 + jnp.exp(-gate)) * up).astype(BF)

    def spread(n, carry):
        left = lax.broadcasted_iota(jnp.int32, (NX, NC, 16, 128), 3) < 64
        for q, tile in ((0, sud[n, :, :, 0, 10]), (1, sg[n, :, :, 10])):
            tile = tile.astype(F32)
            flat = tile.reshape(NX * NC * 16, 128)
            turned = pltpu.roll(flat, 64, 1).reshape(NX, NC, 16, 128)
            ends[q, n, :, :, 0] = jnp.where(left, tile, 0.0).astype(BF)
            ends[q, n, :, :, 1] = jnp.where(left, turned, 0.0).astype(BF)
        return carry

    def message(kind, way, j):
        rows = {"far": 1 - way, "near": way, "comb": 1 - way}[kind]
        to_block = y2 if kind == "far" else (yp, ym)[way]
        src = sums.at[j, way] if kind == "comb" else part.at[j, to_block, pl.ds(rows * HALF, HALF)]
        dst = {"far": far.at[j, way], "near": got.at[j, way], "comb": got.at[j, 2 + way]}[kind]
        return remote(src, dst, rs.at[0], rr.at[j + (0 if kind == "far" else CHUNKS)], (y_next, y_prev)[way])

    def all_far(j):
        return remote(sums.at[j], far.at[j], rs.at[0], rr.at[j], y_next)

    def all_got(j):
        return remote(got.at[j], got.at[j], rs.at[0], rr.at[CHUNKS + j], y_next)

    def second(j):
        def block(n, carry):
            b = (y + 2 + n) % NY
            cols = pl.ds(pl.multiple_of(b * COLS, COLS), COLS)
            part[j, b] = jnp.dot(hid[...], df[:, cols], preferred_element_type=F32).astype(BF)

            @pl.when(n == 0)
            def _():
                for way in range(2):
                    message("far", way, j).start()

            return carry

        lax.fori_loop(0, NY, block, 0)
        for way in range(2):
            message("near", way, j).start()

    def combine(j):
        all_far(j).wait_recv()
        for way in range(2):
            mine = part[j, (yp, ym)[way], pl.ds((1 - way) * HALF, HALF), :].astype(F32)
            sums[j, way] = (mine + far[j, way].astype(F32)).astype(BF)
        for way in range(2):
            message("comb", way, j).start()

    @pl.when(c == 1)
    def _():
        x_end(1, 5, 6, 7)

    with jax.named_scope("normalise_0"):
        normalise(0)
    with jax.named_scope("wait_up"):
        twins(2).wait_recv()
        twins(0).wait_recv()
    with jax.named_scope("first_0"):
        lax.fori_loop(0, NZ, spread, 0)
        first(range(3))

    with jax.named_scope("last_down"):

        @pl.when(c == 0)
        def _():
            x_end(1, 5, 6, 7)

    with jax.named_scope("wait_down"):
        twins(1).wait_recv()

    def assemble(n, carry):
        a, group = n // 4, n % 4
        for s in range(4):
            shard = sud.at[2 * a + group // 2, (group % 2) * 2 + s // 2, s % 2, 1]
            at_row = DROWS * s
            for t in range(4):
                for r in range(2):
                    tmp[pl.ds(at_row + 16 * r, 16), pl.ds(128 * t, 128)] = shard[2 * t + r].astype(F32)
            for p in range(3):
                piece = shard[8 + p].astype(F32)
                tmp[pl.ds(at_row + ROWS, 12), pl.ds(128 * p, 128)] = piece[:12]
                tmp[pl.ds(at_row + ROWS + 4 * p, 4), pl.ds(384, 128)] = piece[12:]
        rows = pl.ds(pl.multiple_of(group * 176, 16), 176)
        df[rows, pl.ds(pl.multiple_of(a * COLS, COLS), COLS)] = tmp[...].astype(BF)
        return carry

    with jax.named_scope("assemble"):
        df[pl.ds(HID, WIDE - HID), :] = jnp.zeros((WIDE - HID, D), BF)
        lax.fori_loop(0, 16, assemble, 0)

    one = lax.broadcasted_iota(jnp.int32, (256, 256), 0) == lax.broadcasted_iota(jnp.int32, (256, 256), 1)
    unit = one.astype(F32).astype(BF)

    def turn_over(quarter):
        to = pl.ds(pl.multiple_of(quarter * 512, 512), 512)
        for n in range(3):
            for q, dst in ((0, ut), (1, gt)):
                dst[pl.ds(256 * n, 256), to] = lax.dot_general(
                    unit, columns(q, n, pl.ds(quarter, 1)), (((1,), (1,)), ((), ())), preferred_element_type=F32
                ).astype(BF)

    def step(j, carry):
        @pl.when(j < CHUNKS)
        def _():
            with jax.named_scope("second"):
                second(j)

        @pl.when(j > 0)
        def _():
            with jax.named_scope("combine"):
                combine(j - 1)

        @pl.when(j < CHUNKS - 1)
        def _():
            with jax.named_scope("first"):
                normalise(j + 1)
                first(range(3))

        @pl.when(jnp.logical_and(j >= 3, j < 7))
        def _():
            with jax.named_scope("turn_over"):
                turn_over(j - 3)

        return carry

    lax.fori_loop(0, CHUNKS + 1, step, 0)

    def finish(j, carry):
        all_got(j).wait_recv()
        for half in range(2):
            mine = part[j, y, pl.ds(half * HALF, HALF), :].astype(F32)
            total = mine + got[j, half].astype(F32) + got[j, 3 - half].astype(F32)
            out[pl.ds(pl.multiple_of(j * CHUNK + half * HALF, HALF), HALF), :] = total.astype(BF)
        return carry

    with jax.named_scope("finish"):
        lax.fori_loop(0, CHUNKS, finish, 0)

    with jax.named_scope("drain"):

        @pl.when(moves)
        def _():
            change.wait_send()

        shards_of(3, gxs.at[0], gxr.at[0]).wait_send()
        far_up.wait_send()
        for way in range(2):
            block = sg.at[pl.ds(0, (6, 7)[way]), x, c]
            remote(block, block, us.at[way], ur.at[0], z_next).wait_send()
            block = sg.at[pl.ds(0, 7), x]
            remote(block, block, gzs.at[way], gzr.at[0], z_next).wait_send()
            remote(tok, xs.at[y], ts.at[way], tr.at[0], y_next).wait_send()
            half = xs.at[0, pl.ds(0, PIECE * PIECES // 2)]
            remote(half, half, tfs.at[way], tfr.at[0], y_next).wait_send()
        block = sg.at[:, :, c]
        remote(block, block, uxs.at[0], uxr.at[0], x_next).wait_send()
        block = sg.at[pl.ds(0, 4), :, c]
        remote(block, block, ufs.at[0], ufr.at[0], x_next).wait_send()
        for n in range(3):
            twins(n).wait_send()
        block = xs.at[pl.ds(0, 3)]
        remote(block, block, rs.at[0], rr.at[0], y_next).wait_send()


def hand_out(gt, ut, df, out, go, uo, do, mo, sem):
    rows = pl.ds(0, HID)
    moved = ((gt.at[rows], go), (ut.at[rows], uo), (df.at[rows], do), (out, mo))
    copies = [pltpu.make_async_copy(src, dst, sem.at[n]) for n, (src, dst) in enumerate(moved)]
    for copy in copies:
        copy.start()
    for copy in copies:
        copy.wait()


def shards(tokens, norm_gain, gate_weight, up_weight, down_weight):
    vmem = functools.partial(pltpu.VMEM, dtype=BF)
    sem = pltpu.SemaphoreType.DMA
    hbm = pl.BlockSpec(memory_space=pltpu.HBM)
    held = pl.pallas_call(
        kernel,
        name="layer",
        out_shape=(jax.ShapeDtypeStruct((WIDE, D), BF),) * 3 + (jax.ShapeDtypeStruct((CHUNK * CHUNKS, COLS), BF),),
        in_specs=[hbm] + [pl.BlockSpec(memory_space=pltpu.VMEM)] * 3,
        out_specs=(pl.BlockSpec(memory_space=pltpu.VMEM),) * 4,
        scratch_shapes=[
            vmem((NY, CHUNK * CHUNKS, COLS)),
            vmem((NZ, NX, NC, TILES, 16, 128)),
            vmem((NZ, NX, NC, 2, TILES, 16, 128)),
            vmem((2, NZ, NX, NC, 2, 16, 128)),
            vmem((TILES, 16, 128)),
            pltpu.VMEM((4 * DROWS, COLS), F32),
            vmem((CHUNK, D)),
            vmem((CHUNK, WIDE)),
            vmem((CHUNKS, NY, CHUNK, COLS)),
            vmem((CHUNKS, 2, HALF, COLS)),
            vmem((CHUNKS, 4, HALF, COLS)),
            vmem((CHUNKS, 2, HALF, COLS)),
            sem((1,)), sem((1,)),
            sem((1,)), sem((3,)),
            sem((2,)), sem((16,)),
            sem((2,)), sem((16,)),
            sem((1,)), sem((32,)),
            sem((1,)), sem((16,)),
            sem((3,)), sem((3,)),
            sem((2,)), sem((2 * PIECES,)),
            sem((2,)), sem((2 * PIECES,)),
            sem((1,)), sem((2 * CHUNKS,)),
            sem((1,)), sem((1,)),
            sem((1,)),
        ],
        compiler_params=pltpu.CompilerParams(collective_id=0, has_side_effects=True, vmem_limit_bytes=LIMIT),
    )(
        tokens,
        (norm_gain[:, None] * gate_weight).astype(BF),
        (norm_gain[:, None] * up_weight).astype(BF),
        down_weight.astype(BF),
    )
    gate, up, down, mixed = pl.pallas_call(
        hand_out,
        name="hand_out",
        out_shape=(jax.ShapeDtypeStruct((HID, D), BF),) * 3 + (jax.ShapeDtypeStruct((CHUNK * CHUNKS, COLS), BF),),
        in_specs=[pl.BlockSpec(memory_space=pl.ANY)] * 4,
        out_specs=(hbm,) * 4,
        scratch_shapes=[sem((4,))],
        compiler_params=pltpu.CompilerParams(vmem_limit_bytes=2**20),
    )(*held)
    return (gate.T, up.T, down, mixed)


def solution(mesh):
    return jax.shard_map(
        shards,
        mesh=mesh,
        in_specs=(P("fs", "tp"), P("fs"), P("fs", "tp"), P("fs", "tp"), P("fs", "tp")),
        out_specs=(P(None, "tp"), P(None, "tp"), P("tp", None), P("fs", "tp")),
        check_vma=False,
    )
```

```python
import functools

import jax
import jax.numpy as jnp
from jax import lax
from jax.experimental import pallas as pl
from jax.experimental.pallas import tpu as pltpu
from jax.sharding import PartitionSpec as P

MESH = pl.DeviceIdType.MESH
BF = jnp.bfloat16
F32 = jnp.float32
NZ, NX, NC, NY = 8, 4, 2, 4
ROWS = 32
HID = 704
WIDE = 768
TILES = 11
DROWS, COLS = 44, 512
D = 2048
CHUNK, CHUNKS = 128, 8
PIECE, PIECES = 256, 4
HALF = CHUNK // 2
EPS = 1e-06
LIMIT = 38 * 2**20


def kernel(
    tok, gw, uw, dw,
    gt, ut, df, out,
    xs, sg, sud, ends, dsend, tmp, xn, hid, part, faraway, got, sums,
    ps, pr, gxs, gxr, gzs, gzr, us, ur, uxs, uxr, ufs, ufr, ds_, dr, ts, tr, tfs, tfr, rs, rr, zfs, zfr, loc,
):
    f, y = lax.axis_index("fs"), lax.axis_index("tp")
    z, x, c = f // 8, (f // 2) % 4, f % 2
    za, zb = z // 2, z % 2

    def at(zz, xx, cc, yy):
        return ((zz * NX + xx) * NC + cc, yy)

    zp, zm = (z + 1) % NZ, (z + 7) % NZ
    xp, xm, x2 = (x + 1) % NX, (x + 3) % NX, (x + 2) % NX
    yp, ym, y2 = (y + 1) % NY, (y + 3) % NY, (y + 2) % NY
    z_next, z_prev = at(zp, x, c, y), at(zm, x, c, y)
    x_next, x_prev, x_far = at(z, xp, c, y), at(z, xm, c, y), at(z, x2, c, y)
    y_next, y_prev = at(z, x, c, yp), at(z, x, c, ym)
    twin, z_far = at(z, x, 1 - c, y), at((z + 4) % NZ, x, c, y)
    pz = 2 * y + zb
    swap = at(pz, x, c, za)
    moves = za != y

    def remote(src, dst, send, recv, device):
        return pltpu.make_async_remote_copy(
            src_ref=src, dst_ref=dst, send_sem=send, recv_sem=recv, device_id=device, device_id_type=MESH
        )

    own_tokens = pltpu.make_async_copy(tok, xs.at[y], loc.at[0])

    barrier = pltpu.get_barrier_semaphore()
    for partner in (z_next, z_prev, z_far, x_next, x_prev, y_next, y_prev, twin):
        pl.semaphore_signal(barrier, inc=1, device_id=partner, device_id_type=MESH)

    @pl.when(moves)
    def _():
        pl.semaphore_signal(barrier, inc=1, device_id=swap, device_id_type=MESH)

    for ref, dst in ((uw, sud.at[z, x, c, 0]), (gw, sg.at[z, x, c])):
        for t in range(5):
            for r in range(2):
                dst[2 * t + r] = ref[pl.ds(16 * r, 16), pl.ds(128 * t, 128)]
        dst[10] = jnp.concatenate([ref[pl.ds(16 * r, 16), pl.ds(640, 64)] for r in range(2)], axis=1)

    def own_down(dst):
        for t in range(4):
            for r in range(2):
                dst[2 * t + r] = dw[pl.ds(16 * r, 16), pl.ds(128 * t, 128)]
        low = dw[pl.ds(ROWS, DROWS - ROWS), :].astype(F32)
        for p in range(3):
            piece = [low[:, 128 * p : 128 * p + 128], low[4 * p : 4 * p + 4, 384:]]
            dst[8 + p] = jnp.concatenate(piece, axis=0).astype(BF)

    @pl.when(moves)
    def _():
        own_down(dsend)

    @pl.when(jnp.logical_not(moves))
    def _():
        own_down(sud.at[z, x, c, 1])

    with jax.named_scope("meet"):
        pl.semaphore_wait(barrier, 8 + moves.astype(jnp.int32))

    change = remote(dsend, sud.at[pz, x, c, 1], ps.at[0], pr.at[0], swap)

    @pl.when(moves)
    def _():
        change.start()

    def token_copy(way, j):
        rows = pl.ds(j * PIECE, PIECE)
        return remote(tok.at[rows], xs.at[y, rows], ts.at[way], tr.at[way * PIECES + j], (y_next, y_prev)[way])

    def token_forward(way, j):
        rows = pl.ds(j * PIECE + way * (PIECE // 2), PIECE // 2)
        block = xs.at[(ym, yp)[way], rows]
        return remote(block, block, tfs.at[way], tfr.at[way * PIECES + j], (y_next, y_prev)[way])

    def token_pass(j):
        for way in range(2):
            token_copy(way, j).wait_recv()
            token_forward(way, j).start()

    for j in range(PIECES):
        for way in range(2):
            token_copy(way, j).start()
    own_tokens.start()

    order = [0, 7, 1, 6, 2, 5, 3, 4]
    last = ((3, 3), (3, 3))

    def came(way, k):
        return (z + (NZ - k if way == 0 else k)) % NZ

    def place(way, k):
        return 7 if k == 4 else 2 * k - 1 + way

    def ud_z(q, way, k):
        block = sud.at[came(way, k), x, c, q]
        return remote(block, block, us.at[way], ur.at[(q * 2 + way) * 4 + k], (z_next, z_prev)[way])

    def ud_x(q, o, way):
        block = sud.at[(z + order[o]) % NZ, x, c, q]
        return remote(block, block, uxs.at[0], uxr.at[(q * 8 + o) * 2 + way], (x_next, x_prev)[way])

    def ud_f(q, o):
        block = sud.at[(z + order[o]) % NZ, (xm, xp)[q], c, q]
        return remote(block, block, ufs.at[0], ufr.at[q * 8 + o], (x_next, x_prev)[q])

    def g_z(way, k, e):
        block = sg.at[came(way, k), (x, xp, xm, x2)[e], c]
        return remote(block, block, gzs.at[way], gzr.at[(way * 4 + k) * 2 + e // 2], (z_next, z_prev)[way])

    def g_pair(way, k, h):
        block = sg.at[came(way, k), pl.ds(0, 2), c]
        return remote(block, block, gzs.at[way], gzr.at[(way * 4 + k) * 2 + h], (z_next, z_prev)[way])

    def g_twin(o, e):
        block = sg.at[(z + order[o]) % NZ, (x, xp, xm, x2)[e], c]
        return remote(block, block, ds_.at[2], dr.at[2], twin)

    def ud_twin(q, o, e):
        block = sud.at[(z + order[o]) % NZ, (x, xp, xm, x2)[e], c, q]
        return remote(block, block, ds_.at[q], dr.at[q], twin)

    def twins(n):
        block = sg.at[:, :, c] if n == 2 else sud.at[:, :, c, n]
        return remote(block, block, ds_.at[n], dr.at[n], twin)

    def ud_arrived(q, o):
        for way in range(2):
            ud_x(q, o, way).start()

    def ud_round(q, k):
        for way in range(2):
            if k <= last[q][way]:
                ud_z(q, way, k - 1).wait_recv()
                if k < last[q][way]:
                    ud_z(q, way, k).start()
                ud_arrived(q, place(way, k))

    def g_round(k, *hs):
        for h in hs:
            for way in range(2):
                if k < 4 or way == 1:
                    g_pair(way, k - 1, h).wait_recv()
                    if k < 3 or k == 3 and way == 1:
                        for e in (2 * h, 2 * h + 1):
                            g_z(way, k, e).start()
                    for e in (2 * h, 2 * h + 1):
                        g_twin(place(way, k), e).start()

    def x_pass(q, *os):
        for o in os:
            for way in (q, 1 - q):
                ud_x(q, o, way).wait_recv()
                if way == q:
                    ud_f(q, o).start()
            for e in range(3):
                ud_twin(q, o, e).start()

    def x_end(q, *os):
        for o in os:
            ud_f(q, o).wait_recv()
            ud_twin(q, o, 3).start()

    def g_x(way):
        block = sg.at[z, x, c]
        return remote(block, block, gxs.at[0], gxr.at[way], (x_next, x_prev)[way])

    def g_far(way):
        block = sg.at[z, (xm, xp)[way], c, (pl.ds(0, 6), pl.ds(6, 5))[way]]
        return remote(block, block, gxs.at[0], gxr.at[2], (x_next, x_prev)[way])

    def shards_of(n, send, recv):
        block = sg.at[z, pl.ds(0, n), c]
        return remote(block, block, send, recv, x_next)

    def far(q):
        block = sud.at[z, x, c, q]
        return remote(block, block, zfs.at[q], zfr.at[q], z_far)

    for way in range(2):
        ud_z(0, way, 0).start()
    for way in range(2):
        g_x(way).start()
    ud_arrived(0, 0)
    far(0).start()
    for way in range(2):
        g_z(way, 0, 0).start()

    with jax.named_scope("change"):

        @pl.when(moves)
        def _():
            change.wait_recv()

    for way in range(2):
        ud_z(1, way, 0).start()
    far(1).start()
    ud_arrived(1, 0)
    with jax.named_scope("round_1"):
        for way in range(2):
            g_x(way).wait_recv()
            g_far(way).start()
        ud_round(0, 1)
        for e in (1, 2):
            for way in range(2):
                g_z(way, 0, e).start()
        x_pass(0, 0)
        far(0).wait_recv()
        ud_arrived(0, 7)
        shards_of(1, gxs.at[0], gxr.at[2]).wait_recv()
        for way in range(2):
            g_z(way, 0, 3).start()
        for e in range(4):
            g_twin(0, e).start()
    with jax.named_scope("round_2"):
        ud_round(0, 2)
        g_round(1, 0)
        ud_round(1, 1)
        x_pass(0, 1, 2, 7)
        far(1).wait_recv()
        ud_arrived(1, 7)
        g_round(1, 1)
        x_pass(1, 0)
        token_pass(0)
    with jax.named_scope("round_3"):
        ud_round(0, 3)
        g_round(2, 0)
        ud_round(1, 2)
        x_pass(0, 3, 4)
        g_round(2, 1)
        x_pass(1, 1, 2, 7)
        x_end(0, 0, 1, 2)
        x_end(1, 0)
    with jax.named_scope("round_4"):
        g_round(3, 0)
        ud_round(1, 3)
        x_pass(0, 5, 6)
        g_round(3, 1)
        token_pass(1)
        x_pass(1, 3, 4)
        x_end(0, 7, 3, 4)
    with jax.named_scope("round_5"):
        g_round(4, 0, 1)
        token_pass(2)
        x_pass(1, 5, 6)
        x_end(0, 5, 6)
        x_end(1, 1, 2, 7)
    with jax.named_scope("round_6"):
        token_pass(3)
        x_end(1, 3, 4)
    own_tokens.wait()

    def normalise(j):
        for k in range(PIECES):

            @pl.when(j == k * (PIECE // CHUNK))
            def _(k=k):
                for way in range(2):
                    token_forward(way, k).wait_recv()

        def rows_of(t, carry):
            rows = pl.ds(pl.multiple_of(j * CHUNK + t * 32, 32), 32)
            total = jnp.zeros((32, 1), F32)
            for b in range(NY):
                v = xs[b, rows, :].astype(F32)
                total = total + jnp.sum(v * v, axis=1, keepdims=True)
            r = lax.rsqrt(total / D + EPS)
            for b in range(NY):
                v = xs[b, rows, :].astype(F32)
                xn[pl.ds(pl.multiple_of(t * 32, 32), 32), pl.ds(b * COLS, COLS)] = (v * r).astype(BF)
            return carry

        lax.fori_loop(0, CHUNK // 32, rows_of, 0)

    def columns(q, n, pairs):
        zs, rows = pl.ds(2 * pairs.start, 2 * pairs.size), pairs.size * D // 4
        halves = []
        for t in (2 * n, 2 * n + 1):
            pair = pl.ds(2 * t, 2)
            if t == 5:
                half = ends[q, zs]
            elif q == 0:
                half = sud[zs, :, :, 0, pair]
            else:
                half = sg[zs, :, :, pair]
            halves.append(half.reshape(rows, 128))
        return jnp.concatenate(halves, axis=1)

    def first(ns):
        for n in ns:
            gate = jnp.dot(xn[...], columns(1, n, pl.ds(0, 4)), preferred_element_type=F32)
            up = jnp.dot(xn[...], columns(0, n, pl.ds(0, 4)), preferred_element_type=F32)
            hid[:, pl.ds(256 * n, 256)] = (gate / (1.0 + jnp.exp(-gate)) * up).astype(BF)

    def spread(n, carry):
        left = lax.broadcasted_iota(jnp.int32, (NX, NC, 16, 128), 3) < 64
        for q, tile in ((0, sud[n, :, :, 0, 10]), (1, sg[n, :, :, 10])):
            tile = tile.astype(F32)
            flat = tile.reshape(NX * NC * 16, 128)
            turned = pltpu.roll(flat, 64, 1).reshape(NX, NC, 16, 128)
            ends[q, n, :, :, 0] = jnp.where(left, tile, 0.0).astype(BF)
            ends[q, n, :, :, 1] = jnp.where(left, turned, 0.0).astype(BF)
        return carry

    def message(kind, way, j):
        rows = {"far": 1 - way, "near": way, "comb": 1 - way}[kind]
        to_block = y2 if kind == "far" else (yp, ym)[way]
        src = sums.at[j, way] if kind == "comb" else part.at[j, to_block, pl.ds(rows * HALF, HALF)]
        dst = {"far": faraway.at[j, way], "near": got.at[j, way], "comb": got.at[j, 2 + way]}[kind]
        return remote(src, dst, rs.at[0], rr.at[j + (0 if kind == "far" else CHUNKS)], (y_next, y_prev)[way])

    def all_far(j):
        return remote(sums.at[j], faraway.at[j], rs.at[0], rr.at[j], y_next)

    def all_got(j):
        return remote(got.at[j], got.at[j], rs.at[0], rr.at[CHUNKS + j], y_next)

    def second(j):
        def block(n, carry):
            b = (y + 2 + n) % NY
            cols = pl.ds(pl.multiple_of(b * COLS, COLS), COLS)
            part[j, b] = jnp.dot(hid[...], df[:, cols], preferred_element_type=F32).astype(BF)

            @pl.when(n == 0)
            def _():
                for way in range(2):
                    message("far", way, j).start()

            return carry

        lax.fori_loop(0, NY, block, 0)
        for way in range(2):
            message("near", way, j).start()

    def combine(j):
        all_far(j).wait_recv()
        for way in range(2):
            mine = part[j, (yp, ym)[way], pl.ds((1 - way) * HALF, HALF), :].astype(F32)
            sums[j, way] = (mine + faraway[j, way].astype(F32)).astype(BF)
        for way in range(2):
            message("comb", way, j).start()

    @pl.when(c == 1)
    def _():
        x_end(1, 5, 6)

    with jax.named_scope("normalise_0"):
        normalise(0)
    with jax.named_scope("wait_up"):
        twins(2).wait_recv()
        twins(0).wait_recv()
    with jax.named_scope("first_0"):
        lax.fori_loop(0, NZ, spread, 0)
        first(range(3))

    with jax.named_scope("last_down"):

        @pl.when(c == 0)
        def _():
            x_end(1, 5, 6)

    with jax.named_scope("wait_down"):
        twins(1).wait_recv()

    def assemble(n, carry):
        a, group = n // 4, n % 4
        for s in range(4):
            shard = sud.at[2 * a + group // 2, (group % 2) * 2 + s // 2, s % 2, 1]
            at_row = DROWS * s
            for t in range(4):
                for r in range(2):
                    tmp[pl.ds(at_row + 16 * r, 16), pl.ds(128 * t, 128)] = shard[2 * t + r].astype(F32)
            for p in range(3):
                piece = shard[8 + p].astype(F32)
                tmp[pl.ds(at_row + ROWS, 12), pl.ds(128 * p, 128)] = piece[:12]
                tmp[pl.ds(at_row + ROWS + 4 * p, 4), pl.ds(384, 128)] = piece[12:]
        rows = pl.ds(pl.multiple_of(group * 176, 16), 176)
        df[rows, pl.ds(pl.multiple_of(a * COLS, COLS), COLS)] = tmp[...].astype(BF)
        return carry

    with jax.named_scope("assemble"):
        df[pl.ds(HID, WIDE - HID), :] = jnp.zeros((WIDE - HID, D), BF)
        lax.fori_loop(0, 16, assemble, 0)

    one = lax.broadcasted_iota(jnp.int32, (256, 256), 0) == lax.broadcasted_iota(jnp.int32, (256, 256), 1)
    unit = one.astype(F32).astype(BF)

    def turn_over(quarter):
        to = pl.ds(pl.multiple_of(quarter * 512, 512), 512)
        for n in range(3):
            for q, dst in ((0, ut), (1, gt)):
                dst[pl.ds(256 * n, 256), to] = lax.dot_general(
                    unit, columns(q, n, pl.ds(quarter, 1)), (((1,), (1,)), ((), ())), preferred_element_type=F32
                ).astype(BF)

    def step(j, carry):
        @pl.when(j < CHUNKS)
        def _():
            with jax.named_scope("second"):
                second(j)

        @pl.when(j > 0)
        def _():
            with jax.named_scope("combine"):
                combine(j - 1)

        @pl.when(j < CHUNKS - 1)
        def _():
            with jax.named_scope("first"):
                normalise(j + 1)
                first(range(3))

        @pl.when(jnp.logical_and(j >= 3, j < 7))
        def _():
            with jax.named_scope("turn_over"):
                turn_over(j - 3)

        return carry

    lax.fori_loop(0, CHUNKS + 1, step, 0)

    def finish(j, carry):
        all_got(j).wait_recv()
        for half in range(2):
            mine = part[j, y, pl.ds(half * HALF, HALF), :].astype(F32)
            total = mine + got[j, half].astype(F32) + got[j, 3 - half].astype(F32)
            out[pl.ds(pl.multiple_of(j * CHUNK + half * HALF, HALF), HALF), :] = total.astype(BF)
        return carry

    with jax.named_scope("finish"):
        lax.fori_loop(0, CHUNKS, finish, 0)

    with jax.named_scope("drain"):

        @pl.when(moves)
        def _():
            change.wait_send()

        shards_of(3, gxs.at[0], gxr.at[0]).wait_send()
        for q in range(2):
            far(q).wait_send()
        for way in range(2):
            block = sg.at[pl.ds(0, 6), x, c]
            remote(block, block, us.at[way], ur.at[0], z_next).wait_send()
            block = sg.at[pl.ds(0, (6, 8)[way]), x]
            remote(block, block, gzs.at[way], gzr.at[0], z_next).wait_send()
            remote(tok, xs.at[y], ts.at[way], tr.at[0], y_next).wait_send()
            half = xs.at[0, pl.ds(0, PIECE * PIECES // 2)]
            remote(half, half, tfs.at[way], tfr.at[0], y_next).wait_send()
        block = sg.at[:, :, c]
        remote(block, block, uxs.at[0], uxr.at[0], x_next).wait_send()
        block = sg.at[pl.ds(0, 4), :, c]
        remote(block, block, ufs.at[0], ufr.at[0], x_next).wait_send()
        for n in range(3):
            twins(n).wait_send()
        block = xs.at[pl.ds(0, 3)]
        remote(block, block, rs.at[0], rr.at[0], y_next).wait_send()


def hand_out(gt, ut, df, out, go, uo, do, mo, sem):
    rows = pl.ds(0, HID)
    moved = ((gt.at[rows], go), (ut.at[rows], uo), (df.at[rows], do), (out, mo))
    copies = [pltpu.make_async_copy(src, dst, sem.at[n]) for n, (src, dst) in enumerate(moved)]
    for copy in copies:
        copy.start()
    for copy in copies:
        copy.wait()


def shards(tokens, norm_gain, gate_weight, up_weight, down_weight):
    vmem = functools.partial(pltpu.VMEM, dtype=BF)
    sem = pltpu.SemaphoreType.DMA
    hbm = pl.BlockSpec(memory_space=pltpu.HBM)
    held = pl.pallas_call(
        kernel,
        name="layer",
        out_shape=(jax.ShapeDtypeStruct((WIDE, D), BF),) * 3 + (jax.ShapeDtypeStruct((CHUNK * CHUNKS, COLS), BF),),
        in_specs=[hbm] + [pl.BlockSpec(memory_space=pltpu.VMEM)] * 3,
        out_specs=(pl.BlockSpec(memory_space=pltpu.VMEM),) * 4,
        scratch_shapes=[
            vmem((NY, CHUNK * CHUNKS, COLS)),
            vmem((NZ, NX, NC, TILES, 16, 128)),
            vmem((NZ, NX, NC, 2, TILES, 16, 128)),
            vmem((2, NZ, NX, NC, 2, 16, 128)),
            vmem((TILES, 16, 128)),
            pltpu.VMEM((4 * DROWS, COLS), F32),
            vmem((CHUNK, D)),
            vmem((CHUNK, WIDE)),
            vmem((CHUNKS, NY, CHUNK, COLS)),
            vmem((CHUNKS, 2, HALF, COLS)),
            vmem((CHUNKS, 4, HALF, COLS)),
            vmem((CHUNKS, 2, HALF, COLS)),
            sem((1,)), sem((1,)),
            sem((1,)), sem((3,)),
            sem((2,)), sem((16,)),
            sem((2,)), sem((16,)),
            sem((1,)), sem((32,)),
            sem((1,)), sem((16,)),
            sem((3,)), sem((3,)),
            sem((2,)), sem((2 * PIECES,)),
            sem((2,)), sem((2 * PIECES,)),
            sem((1,)), sem((2 * CHUNKS,)),
            sem((2,)), sem((2,)),
            sem((1,)),
        ],
        compiler_params=pltpu.CompilerParams(collective_id=0, has_side_effects=True, vmem_limit_bytes=LIMIT),
    )(
        tokens,
        (norm_gain[:, None] * gate_weight).astype(BF),
        (norm_gain[:, None] * up_weight).astype(BF),
        down_weight.astype(BF),
    )
    gate, up, down, mixed = pl.pallas_call(
        hand_out,
        name="hand_out",
        out_shape=(jax.ShapeDtypeStruct((HID, D), BF),) * 3 + (jax.ShapeDtypeStruct((CHUNK * CHUNKS, COLS), BF),),
        in_specs=[pl.BlockSpec(memory_space=pl.ANY)] * 4,
        out_specs=(hbm,) * 4,
        scratch_shapes=[sem((4,))],
        compiler_params=pltpu.CompilerParams(vmem_limit_bytes=2**20),
    )(*held)
    return (gate.T, up.T, down, mixed)


def solution(mesh):
    return jax.shard_map(
        shards,
        mesh=mesh,
        in_specs=(P("fs", "tp"), P("fs"), P("fs", "tp"), P("fs", "tp"), P("fs", "tp")),
        out_specs=(P(None, "tp"), P(None, "tp"), P("tp", None), P("fs", "tp")),
        check_vma=False,
    )
```
